32 devices in a mesh: sp: 4 (over z), fs: 4 (over y, core), tp: 2 (over x).
Axes of the slice: x: 2, y: 2, z: 4, core: 2. Of those that a mesh axis runs over, the one named last changes fastest.
Arguments:
- tokens: bfloat16 [8, 2048, 2048], P('fs', ('sp', 'tp')), may hold values from -6 to 6
- norm_gain: float32 [2048], replicated, may hold values from 0.1 to 1.9
- w_pool_in: bfloat16 [2048, 1024], P('fs', 'tp'), may hold values from -0.125 to 0.125
- pool_mix: bfloat16 [8, 128, 128], replicated, may hold values from -0.5 to 0.5
- pool_scale: float32 [1024], replicated, may hold values from 0.1 to 1.9
- w_query: bfloat16 [2048, 1024], P('fs', 'tp'), may hold values from -0.13258252 to 0.13258252
- w_key: bfloat16 [2048, 1024], P('fs', 'tp'), may hold values from -0.508233 to 0.508233
- w_value: bfloat16 [2048, 1024], P('fs', 'tp'), may hold values from -0.125 to 0.125
- gate_cache: float32 [8, 8, 2048], P('fs', 'tp'), may hold values from -258 to 0, as said below
- w_out_pool: bfloat16 [1024, 2048], P('tp', 'fs'), may hold values from -0.125 to 0.125
- w_out_attn: bfloat16 [1024, 2048], P('tp', 'fs'), may hold values from -0.75 to 0.75
Outputs:
- mixed: bfloat16 [8, 2048, 2048], P('fs', ('sp', 'tp'))
The draws below stay inside these ranges and needn't reach their ends.
Inputs may be any that keep to these rules, and one draw needn't show every extreme that they name: `gate_cache`: each head's values never rise along the positions.
All inputs are finite; a program needn't handle non-finite values.
Results may differ from the reference program's by a relative error of at most 0.014.
Values may be sent and summed in bfloat16 or wider, within the bound.
A program may use at most 128 MiB of HBM per device.

```python
import jax
import jax.numpy as jnp
from jax import lax

D = 2048
HEAD_DIM = 128
HEAD_TOTAL = 8
GROUPS = 8
GROUP_WIDTH = 128
POOL_WIDTH = 1024
ATTN_WIDTH = 1024
TOK_DEV = 512
SEQUENCE_LENGTH = 2048
SEQUENCE_TOTAL = 8
N_TP = 2


def query_key_pair(key):
    joined = jax.random.fold_in(key, 4242)
    first_key, second_key = jax.random.split(joined)
    query_part = jnp.clip(jax.random.normal(first_key, (D, ATTN_WIDTH), jnp.float32), -6.0, 6.0)
    key_part = jnp.clip(jax.random.normal(second_key, (D, ATTN_WIDTH), jnp.float32), -6.0, 6.0)
    return (query_part * D ** (-0.5), key_part * D ** (-0.5))


def draw_w_query(key, part):
    return query_key_pair(key)[0].astype(jnp.bfloat16)


def draw_w_key(key, part):
    return query_key_pair(key)[1].astype(jnp.bfloat16)


def draw_gate_cache(key, part):
    joined = jax.random.fold_in(key, 917)
    sequence_flows = jax.random.split(joined, 7)
    block_count = SEQUENCE_LENGTH // TOK_DEV
    ranking = jax.vmap(lambda single: jax.random.permutation(single, HEAD_TOTAL))(jax.random.split(sequence_flows[0], SEQUENCE_TOTAL))
    fast_count = HEAD_TOTAL // 2
    rapid_decay = ranking < fast_count
    quick_rate = jnp.exp(jax.random.uniform(sequence_flows[1], (SEQUENCE_TOTAL, HEAD_TOTAL), jnp.float32, jnp.log(1.0 / 100.0), jnp.log(1.0 / 30.0)))
    slow_total = jnp.exp(jax.random.uniform(sequence_flows[2], (SEQUENCE_TOTAL, HEAD_TOTAL), jnp.float32, jnp.log(0.15), jnp.log(0.5)))
    baseline_rate = jnp.where(rapid_decay, quick_rate, slow_total / SEQUENCE_LENGTH)
    block_factor = jnp.exp(jax.random.uniform(sequence_flows[3], (SEQUENCE_TOTAL, HEAD_TOTAL, block_count), jnp.float32, jnp.log(0.5), jnp.log(2.0)))
    position_multiplier = jnp.repeat(block_factor, TOK_DEV, axis=2)
    jitter_level = jax.random.uniform(sequence_flows[4], (SEQUENCE_TOTAL, HEAD_TOTAL, SEQUENCE_LENGTH), jnp.float32, 0.2, 1.8)
    spike_locations = jax.random.randint(sequence_flows[5], (SEQUENCE_TOTAL, HEAD_TOTAL, 2), 0, SEQUENCE_LENGTH)
    spike_depth = jax.random.uniform(sequence_flows[6], (SEQUENCE_TOTAL, HEAD_TOTAL, 2), jnp.float32, 0.22, 0.6)
    token_positions = jnp.arange(SEQUENCE_LENGTH)
    spike_hits = token_positions[None, None, None, :] == spike_locations[:, :, :, None]
    spike_events = jnp.sum(jnp.where(spike_hits, spike_depth[:, :, :, None], 0.0), axis=2)
    spike_events = jnp.where(rapid_decay[:, :, None], 0.0, spike_events)
    step_increments = baseline_rate[:, :, None] * position_multiplier * jitter_level + spike_events
    return -jnp.cumsum(step_increments, axis=2)


def block_scale(own_key, extent, shards, smallest, top_value):
    def one(dim, shards_of):
        steps = jax.random.uniform(jax.random.fold_in(jax.random.fold_in(own_key, 6), dim), (shards_of,), jnp.float32, smallest / len(shards), top_value / len(shards))
        return jnp.repeat(jnp.exp(steps), extent[dim] // shards_of).reshape((-1,) + (1,) * (len(extent) - dim - 1))

    gain = one(*shards[0])
    for cut in shards[1:]:
        gain = gain * one(*cut)
    return gain


def centred(rng, extent, scale, most, cuts=(), kind=jnp.bfloat16):
    result = jax.random.normal(rng, extent, jnp.float32) * scale
    if len(cuts) > 0:
        result = block_scale(rng, extent, cuts, -0.22, 0.18) * result
    return jnp.clip(result, min=-most, max=most).astype(kind)


def setup_inputs(seed: int = 0) -> dict:
    key_of = jax.random.split(jax.random.key(seed), 12)
    return {
        "tokens": centred(key_of[0], (SEQUENCE_TOTAL, SEQUENCE_LENGTH, D), 1.0, 6.0, ((0, 4), (1, 8))),
        "norm_gain": jnp.clip(1.0 + 0.18 * jax.random.normal(key_of[1], (D,), jnp.float32), 0.1, 1.9),
        "w_pool_in": centred(key_of[2], (D, POOL_WIDTH), D ** -0.5, 0.125, ((0, 4), (1, 2))),
        "pool_mix": centred(key_of[3], (GROUPS, GROUP_WIDTH, GROUP_WIDTH), GROUP_WIDTH ** -0.5, 0.5),
        "pool_scale": jnp.clip(1.0 + 0.18 * jax.random.normal(key_of[4], (POOL_WIDTH,), jnp.float32), 0.1, 1.9),
        "w_query": draw_w_query(jax.random.fold_in(key_of[11], 71), 0),
        "w_key": draw_w_key(jax.random.fold_in(key_of[11], 71), 0),
        "w_value": centred(key_of[7], (D, ATTN_WIDTH), D ** -0.5, 0.125, ((0, 4), (1, 2))),
        "gate_cache": draw_gate_cache(jax.random.fold_in(key_of[11], 71), 0),
        "w_out_pool": centred(key_of[9], (POOL_WIDTH, D), (POOL_WIDTH + ATTN_WIDTH) ** -0.5, 0.125, ((0, 2), (1, 4))),
        "w_out_attn": centred(key_of[10], (ATTN_WIDTH, D), (ATTN_WIDTH // 16) ** -0.5, 0.75, ((0, 2), (1, 4))),
    }


norm_eps = 1e-06
widest = 16

def settle(values):
    return lax.optimization_barrier(values.astype(jnp.bfloat16))

def window_sums(extended):
    outcome = []
    current = extended
    offset = 1
    for doubling in range(4):
        padding = jnp.zeros((offset, extended.shape[1]), extended.dtype)
        current = current + jnp.concatenate([padding, current[:-offset]], axis=0)
        offset = offset * 2
        outcome.append(current[widest - 1:])
    return outcome

def pool_branch(projected, mixing, scaling):
    row_count = projected.shape[0]
    channels = projected.shape[1]
    border = jnp.zeros((widest - 1, channels), jnp.float32)
    widened = projected.astype(jnp.float32)
    totals = window_sums(jnp.concatenate([border, widened], axis=0))
    token_positions = jnp.arange(row_count)
    window_index = jnp.arange(channels) // GROUP_WIDTH % 4
    averaged = jnp.zeros((row_count, channels), jnp.float32)
    for doubling in range(4):
        counted = jnp.minimum(token_positions + 1, 2 ** (doubling + 1)).astype(jnp.float32)
        picked = (window_index == doubling).astype(jnp.float32)
        averaged = averaged + picked[None, :] * totals[doubling] / counted[:, None]
    departure = settle(averaged - widened).astype(jnp.float32)
    mixed_rows = jnp.einsum('tgc,gcd->tgd', departure.reshape(row_count, GROUPS, GROUP_WIDTH), mixing.astype(jnp.float32))
    return (mixed_rows.reshape(row_count, channels) * scaling[None, :]).astype(jnp.bfloat16)

def attention(query_proj, key_proj, value_proj, gate_rows):
    row_count = query_proj.shape[0]
    block_rows = 512 if row_count % 512 == 0 else row_count
    shaped = (row_count, HEAD_TOTAL, HEAD_DIM)
    query_heads = query_proj.reshape(shaped).astype(jnp.float32)
    key_heads = key_proj.reshape(shaped).astype(jnp.float32)
    value_heads = value_proj.reshape(shaped).astype(jnp.float32)
    gate_cols = jnp.transpose(gate_rows)
    pieces = []
    for query_start in range(0, row_count, block_rows):
        query_end = query_start + block_rows
        scores = jnp.einsum('qhd,khd->qhk', query_heads[query_start:query_end], key_heads[:query_end]) * HEAD_DIM ** (-0.5)
        scores = scores + gate_cols[query_start:query_end, :, None] - gate_rows[None, :, :query_end]
        allowed = (jnp.arange(query_end)[None, :] <= jnp.arange(query_start, query_end)[:, None])[:, None, :]
        scores = jnp.where(allowed, scores, -jnp.inf)
        highest = lax.optimization_barrier(jnp.max(scores, axis=2, keepdims=True))
        lifted = jnp.exp(scores - highest)
        denominator = lax.optimization_barrier(jnp.sum(lifted, axis=2))
        rounded = settle(lifted).astype(jnp.float32)
        weighted = jnp.einsum('qhk,khd->qhd', rounded, value_heads[:query_end])
        pieces.append((weighted / denominator[:, :, None]).astype(jnp.bfloat16))
    return jnp.concatenate(pieces, axis=0).reshape(row_count, HEAD_TOTAL * HEAD_DIM)

def reference(tokens, norm_gain, w_pool_in, pool_mix, pool_scale, w_query, w_key, w_value, gate_cache, w_out_pool, w_out_attn):
    pool_share = POOL_WIDTH // N_TP
    attn_share = ATTN_WIDTH // N_TP
    outputs = []
    for sequence in range(SEQUENCE_TOTAL):
        widened = tokens[sequence].astype(jnp.float32)
        normed = (widened * lax.rsqrt(lax.optimization_barrier(jnp.mean(widened * widened, axis=-1, keepdims=True)) + norm_eps) * norm_gain[None, :]).astype(jnp.bfloat16)
        pool_in = settle(jnp.dot(normed, w_pool_in, preferred_element_type=jnp.float32))
        query_proj = settle(jnp.dot(normed, w_query, preferred_element_type=jnp.float32))
        key_proj = settle(jnp.dot(normed, w_key, preferred_element_type=jnp.float32))
        value_proj = settle(jnp.dot(normed, w_value, preferred_element_type=jnp.float32))
        pool_out = pool_branch(pool_in, pool_mix, pool_scale)
        attn_out = attention(query_proj, key_proj, value_proj, gate_cache[sequence])
        summed = jnp.zeros((SEQUENCE_LENGTH, D), jnp.float32)
        for member in range(N_TP):
            pool_lo = member * pool_share
            attn_lo = member * attn_share
            partial_value = jnp.dot(pool_out[:, pool_lo:pool_lo + pool_share], w_out_pool[pool_lo:pool_lo + pool_share], preferred_element_type=jnp.float32)
            partial_value = partial_value + jnp.dot(attn_out[:, attn_lo:attn_lo + attn_share], w_out_attn[attn_lo:attn_lo + attn_share], preferred_element_type=jnp.float32)
            summed = summed + settle(partial_value).astype(jnp.float32)
        outputs.append(summed.astype(jnp.bfloat16))
    return jnp.stack(outputs, axis=0)
```

```python
import jax
import jax.numpy as jnp
from jax import lax
from jax.experimental import pallas as pl
from jax.experimental.pallas import tpu as pltpu
from jax.sharding import PartitionSpec as P

HEAD_DIM = 128
GROUP_WIDTH = 128


norm_eps = 1e-06
widest = 16
masked_score = -1e30


def shifted(x, axis, by):
    length = lax.axis_size(axis)
    pairs = [(i, i + by) for i in range(length) if 0 <= i + by < length]
    return lax.ppermute(x, axis, pairs)


def window_sums(extended):
    outcome = []
    current = extended
    offset = 1
    for doubling in range(4):
        padding = jnp.zeros((offset, extended.shape[1]), jnp.float32)
        current = current + jnp.concatenate([padding, current[:-offset]], axis=0)
        offset = offset * 2
        outcome.append(current[widest - 1 :])
    return outcome


def pool_branch(projected, border, first_group, first_position, mixing, scaling):
    row_count = projected.shape[0]
    channels = projected.shape[1]
    widened = projected.astype(jnp.float32)
    totals = window_sums(jnp.concatenate([border.astype(jnp.float32), widened], axis=0))
    token_positions = first_position + jnp.arange(row_count)
    window_index = (first_group + jnp.arange(channels) // GROUP_WIDTH) % 4
    averaged = jnp.zeros((row_count, channels), jnp.float32)
    for doubling in range(4):
        counted = jnp.minimum(token_positions + 1, 2 ** (doubling + 1)).astype(jnp.float32)
        picked = (window_index == doubling).astype(jnp.float32)
        averaged = averaged + picked[None, :] * totals[doubling] / counted[:, None]
    departure = (averaged - widened).astype(jnp.bfloat16)
    group_count = channels // GROUP_WIDTH
    mixed_rows = jnp.einsum(
        "tgc,gcd->tgd",
        departure.reshape(row_count, group_count, GROUP_WIDTH),
        mixing,
        preferred_element_type=jnp.float32,
    )
    return (mixed_rows.reshape(row_count, channels) * scaling[None, :]).astype(jnp.bfloat16)


def general_device(
    tokens,
    norm_gain,
    w_pool_in,
    pool_mix,
    pool_scale,
    w_query,
    w_key,
    w_value,
    gate_cache,
    w_out_pool,
    w_out_attn,
):
    tp_index = lax.axis_index("tp")
    tp_count = lax.axis_size("tp")
    seq_count = tokens.shape[0]
    own_count = tokens.shape[1]
    token_count = own_count * tp_count
    first_position = lax.axis_index("sp") * token_count
    own_rows = tokens.astype(jnp.float32)
    normed = (
        own_rows
        * lax.rsqrt(jnp.mean(own_rows * own_rows, axis=-1, keepdims=True) + norm_eps)
        * norm_gain[None, None, :]
    ).astype(jnp.bfloat16)
    pool_full, query_full, key_full, value_full, out_pool_full, out_attn_full = (
        lax.all_gather(w_pool_in, "fs", axis=0, tiled=True),
        lax.all_gather(w_query, "fs", axis=0, tiled=True),
        lax.all_gather(w_key, "fs", axis=0, tiled=True),
        lax.all_gather(w_value, "fs", axis=0, tiled=True),
        lax.all_gather(w_out_pool, "fs", axis=1, tiled=True),
        lax.all_gather(w_out_attn, "fs", axis=1, tiled=True),
    )
    pool_cols = w_pool_in.shape[1]
    attn_cols = w_query.shape[1]
    shard_rows = lax.all_gather(normed, "tp", axis=1, tiled=True)
    projected = jnp.concatenate(
        [
            jnp.dot(shard_rows, pool_full, preferred_element_type=jnp.float32).astype(jnp.bfloat16),
            jnp.dot(shard_rows, query_full, preferred_element_type=jnp.float32).astype(
                jnp.bfloat16
            ),
            jnp.dot(shard_rows, key_full, preferred_element_type=jnp.float32).astype(jnp.bfloat16),
            jnp.dot(shard_rows, value_full, preferred_element_type=jnp.float32).astype(
                jnp.bfloat16
            ),
        ],
        axis=2,
    )
    pool_in = projected[:, :, :pool_cols]
    query_proj = projected[:, :, pool_cols : pool_cols + attn_cols]
    key_proj = projected[:, :, pool_cols + attn_cols : pool_cols + 2 * attn_cols]
    value_proj = projected[:, :, pool_cols + 2 * attn_cols :]
    group_local = pool_cols // GROUP_WIDTH
    mixing = lax.dynamic_slice_in_dim(pool_mix, tp_index * group_local, group_local, 0)
    scaling = lax.dynamic_slice_in_dim(pool_scale, tp_index * pool_cols, pool_cols, 0)
    borders = shifted(pool_in[:, token_count - (widest - 1) :], "sp", 1)
    pool_out = jnp.stack(
        [
            pool_branch(
                pool_in[member],
                borders[member],
                tp_index * group_local,
                first_position,
                mixing,
                scaling,
            )
            for member in range(seq_count)
        ],
        axis=0,
    )
    head_count = attn_cols // HEAD_DIM
    query_heads = query_proj.reshape(seq_count, token_count, head_count, HEAD_DIM)
    query_gates = jnp.transpose(
        lax.dynamic_slice_in_dim(gate_cache, first_position, token_count, 2), (0, 2, 1)
    )
    query_positions = first_position + jnp.arange(token_count)
    last_position = first_position + token_count - 1
    score_scale = HEAD_DIM ** (-0.5)
    start_state = (
        jnp.full((seq_count, token_count, head_count), masked_score, jnp.float32),
        jnp.zeros((seq_count, token_count, head_count), jnp.float32),
        jnp.zeros((seq_count, token_count, head_count, HEAD_DIM), jnp.float32),
    )
    key_shard = lax.all_gather(key_proj, "sp", axis=1, tiled=True)
    value_shard = lax.all_gather(value_proj, "sp", axis=1, tiled=True)
    key_total = key_shard.shape[1]
    block_rows = 512

    def one_block(block_state, block_index):
        key_start = block_index * block_rows

        def compute(inner_state):
            running_top, running_sum, running_out = inner_state
            key_block = lax.dynamic_slice_in_dim(key_shard, block_index * block_rows, block_rows, 1)
            value_block = lax.dynamic_slice_in_dim(
                value_shard, block_index * block_rows, block_rows, 1
            )
            key_block = key_block.reshape(seq_count, block_rows, head_count, HEAD_DIM)
            value_block = value_block.reshape(seq_count, block_rows, head_count, HEAD_DIM)
            key_gates = lax.dynamic_slice_in_dim(gate_cache, key_start, block_rows, 2)
            scores = (
                jnp.einsum(
                    "sqhd,skhd->sqhk", query_heads, key_block, preferred_element_type=jnp.float32
                )
                * score_scale
            )
            scores = scores + query_gates[:, :, :, None] - key_gates[:, None, :, :]
            allowed = ((key_start + jnp.arange(block_rows))[None, :] <= query_positions[:, None])[
                None, :, None, :
            ]
            scores = jnp.where(allowed, scores, masked_score)
            new_top = jnp.maximum(running_top, jnp.max(scores, axis=3))
            weights = jnp.where(allowed, jnp.exp(scores - new_top[:, :, :, None]), 0.0)
            shrink = jnp.exp(running_top - new_top)
            running_sum = running_sum * shrink + jnp.sum(weights, axis=3)
            running_out = running_out * shrink[:, :, :, None] + jnp.einsum(
                "sqhk,skhd->sqhd",
                weights.astype(jnp.bfloat16),
                value_block,
                preferred_element_type=jnp.float32,
            )
            return (new_top, running_sum, running_out)

        def unchanged(inner_state):
            return inner_state

        return (lax.cond(key_start <= last_position, compute, unchanged, block_state), None)

    result, unused = lax.scan(one_block, start_state, jnp.arange(key_total // block_rows))
    final_top, final_sum, final_out = result
    attn_out = (
        (final_out / final_sum[:, :, :, None])
        .astype(jnp.bfloat16)
        .reshape(seq_count, token_count, attn_cols)
    )
    pool_flat = jnp.transpose(
        pool_out.reshape(seq_count, tp_count, own_count, pool_cols), (1, 0, 2, 3)
    ).reshape(tp_count * seq_count * own_count, pool_cols)
    attn_flat = jnp.transpose(
        attn_out.reshape(seq_count, tp_count, own_count, attn_cols), (1, 0, 2, 3)
    ).reshape(tp_count * seq_count * own_count, attn_cols)
    summed = lax.psum_scatter(
        (
            jnp.dot(pool_flat, out_pool_full, preferred_element_type=jnp.float32)
            + jnp.dot(attn_flat, out_attn_full, preferred_element_type=jnp.float32)
        ).astype(jnp.bfloat16),
        "tp",
        scatter_dimension=0,
        tiled=True,
    ).astype(jnp.float32)
    return summed.astype(jnp.bfloat16).reshape(seq_count, own_count, summed.shape[1])


log2_e = 1.4426950408889634
MESH = pl.DeviceIdType.MESH
KEY, VALUE, QUERY, POOL = 0, 1, 2, 3


def layer_kernel(
    tokens,
    gain,
    w_pool,
    mix,
    scale,
    w_query,
    w_key,
    w_value,
    gates,
    w_out_pool,
    w_out_attn,
    out,
    w_in,
    w_out,
    rows_ref,
    stage,
    heads,
    extended,
    border_out,
    border_in,
    pool_tmp,
    pool_rows,
    attn_own,
    attn_rows,
    out_stage,
    local_sem,
    send_sem,
    recv_sem,
    attn_send,
    attn_recv,
):
    z = lax.axis_index("sp")
    f = lax.axis_index("fs")
    x = lax.axis_index("tp")
    seqs, half, width = tokens.shape
    block = 2 * half
    depth, cols = w_key.shape
    other_x = 1 - x
    sibling = f + 1 - 2 * lax.rem(f, 2)
    across = lax.rem(f + 2, 4)
    z_count = stage.shape[3]

    def z_at(by):
        return lax.rem(z + by, z_count)

    barrier = pltpu.get_barrier_semaphore()
    peers = [{"tp": other_x}, {"fs": sibling}, {"fs": across}]
    for by in range(1, z_count):
        peers.append({"sp": z_at(by)})
        peers.append({"sp": z_at(by), "tp": other_x})
    for peer in peers:
        pl.semaphore_signal(barrier, inc=1, device_id=peer, device_id_type=MESH)
    pl.semaphore_wait(barrier, len(peers))

    numbers = iter(range(send_sem.shape[0]))

    def remote(source, target, peer):
        number = next(numbers)
        return pltpu.make_async_remote_copy(
            src_ref=source,
            dst_ref=target,
            send_sem=send_sem.at[number],
            recv_sem=recv_sem.at[number],
            device_id=peer,
            device_id_type=MESH,
        )

    local_numbers = iter(range(local_sem.shape[0]))

    def local(source, target):
        return pltpu.make_async_copy(source, target, local_sem.at[next(local_numbers)])

    def in_slot(kind, owner):
        return w_in.at[kind, pl.ds(pl.multiple_of(owner * depth, depth), depth)]

    def out_slot(kind, owner_x, owner_f):
        return w_out.at[
            kind,
            pl.ds(pl.multiple_of(owner_x * cols, cols), cols),
            pl.ds(pl.multiple_of(owner_f * depth, depth), depth),
        ]

    w_own = (w_key, w_value, w_query, w_pool)
    out_own = (w_out_pool, w_out_attn)
    kinds = range(4)

    tok_x = [remote(tokens.at[s], rows_ref.at[s, 1], {"tp": other_x}) for s in range(seqs)]
    in_y = [remote(w_own[k], in_slot(k, f), {"fs": across}) for k in kinds]
    in_sib = [remote(w_own[k], in_slot(k, f), {"fs": sibling}) for k in kinds]
    in_corner = [remote(in_slot(k, across), in_slot(k, across), {"fs": sibling}) for k in kinds]
    out_x = [remote(out_own[k], out_slot(k, x, f), {"tp": other_x}) for k in range(2)]
    out_y = [remote(out_own[k], out_slot(k, x, f), {"fs": across}) for k in range(2)]
    out_sib = [remote(out_own[k], out_slot(k, x, f), {"fs": sibling}) for k in range(2)]

    def forwarded(owner_x, owner_f, peer):
        return [
            remote(out_slot(k, owner_x, owner_f), out_slot(k, owner_x, owner_f), peer)
            for k in range(2)
        ]

    out_xy = forwarded(other_x, f, {"fs": across})
    out_xs = forwarded(other_x, f, {"fs": sibling})
    out_ys = forwarded(x, across, {"fs": sibling})
    out_xys = forwarded(other_x, across, {"fs": sibling})
    tok_local = [local(tokens.at[s], rows_ref.at[s, 0]) for s in range(seqs)]
    in_local = [local(w_own[k], in_slot(k, f)) for k in kinds]
    out_local = [local(out_own[k], out_slot(k, x, f)) for k in range(2)]

    def start(copies):
        for copy in copies:
            copy.start()

    def arrive(copies):
        for copy in copies:
            copy.wait_recv()

    tok_x[0].start()
    start(in_y)
    start(tok_x[1:])
    start(tok_local)
    for k in kinds:
        in_local[k].start()
        in_sib[k].start()

    def normalize(s, which):
        step_rows = 64

        def step(i, carry):
            at = pl.ds(pl.multiple_of(i * step_rows, step_rows), step_rows)
            values = rows_ref[s, which, at].astype(jnp.float32)
            mean = jnp.mean(values * values, axis=-1, keepdims=True)
            rows_ref[s, which, at] = (
                values * lax.rsqrt(mean + norm_eps) * gain[...]
            ).astype(jnp.bfloat16)
            return carry

        lax.fori_loop(0, half // step_rows, step, 0)

    def project(s, which, kind):
        return jnp.dot(
            rows_ref[s, which], w_in[kind], preferred_element_type=jnp.float32
        ).astype(jnp.bfloat16)

    def stage_heads(s, which, kind):
        result = project(s, which, kind)
        for h in range(z_count):
            stage[which, kind, s, h] = result[:, h * HEAD_DIM : (h + 1) * HEAD_DIM]

    def span(owner_z, owner_x):
        return pl.ds(pl.multiple_of(owner_z * block + owner_x * half, half), half)

    for copy in tok_local:
        copy.wait()
    for s in range(seqs):
        normalize(s, 0)

    def weights_ready(k):
        in_local[k].wait()
        in_sib[k].wait_recv()
        in_y[k].wait_recv()
        in_corner[k].start()
        in_corner[k].wait_recv()

    own_copies = []
    for kind in (KEY, VALUE, QUERY):
        weights_ready(kind)

        def own_step(s, carry, kind=kind):
            stage_heads(s, 0, kind)
            heads[kind, s, span(z, x)] = stage[0, kind, s, z]
            return carry

        lax.fori_loop(0, seqs, own_step, 0)
        for by in range(z_count - 1, 0, -1):
            copy = remote(
                stage.at[0, kind, :, z_at(by)],
                heads.at[kind, :, span(z, x)],
                {"sp": z_at(by)},
            )
            copy.start()
            own_copies.append(copy)

    other_copies = []
    for s in range(seqs):
        tok_x[s].wait_recv()
        normalize(s, 1)

        def other_step(kind, carry, s=s):
            stage_heads(s, 1, kind)
            heads[kind, s, span(z, other_x)] = stage[1, kind, s, z]
            return carry

        lax.fori_loop(0, 3, other_step, 0)
        group = []
        for by in range(z_count - 1, 0, -1):
            copy = remote(
                stage.at[1, :, s, z_at(by)],
                heads.at[:, s, span(z, other_x)],
                {"sp": z_at(by)},
            )
            copy.start()
            group.append(copy)
        other_copies.append(group)

    start(out_x)
    weights_ready(POOL)
    start(out_y)
    start(out_sib)
    start(out_local)

    edge = border_out.shape[1]
    for s in range(seqs):
        for which, owner in ((0, x), (1, other_x)):
            at = pl.multiple_of(edge + owner * half, edge)
            extended[s, pl.ds(at, half)] = project(s, which, POOL).astype(jnp.float32)
        border_out[s] = extended[s, block:].astype(jnp.bfloat16)

    border = remote(border_out, border_in, {"sp": z_at(1)})

    @pl.when(z < z_count - 1)
    def send_border():
        border.start()

    @pl.when(z > 0)
    def take_border():
        border.wait_recv()
        extended[:, 0:edge] = border_in[...].astype(jnp.float32)

    @pl.when(z == 0)
    def no_border():
        extended[:, 0:edge] = jnp.zeros((seqs, edge, cols), jnp.float32)

    groups = cols // GROUP_WIDTH
    pool_copies = []
    for s in range(seqs):
        seen = (
            z * block + lax.broadcasted_iota(jnp.int32, (block, GROUP_WIDTH), 0) + 1
        ).astype(jnp.float32)
        for g in range(groups):
            at = slice(g * GROUP_WIDTH, (g + 1) * GROUP_WIDTH)
            plain = extended[s, :, at]
            total = plain
            for doubling in range(g + 1):
                total = total + pltpu.roll(total, 2**doubling, 0)
            averaged = total[edge:] / jnp.minimum(seen, float(2 ** (g + 1)))
            departure = (averaged - plain[edge:]).astype(jnp.bfloat16)
            mixed = jnp.dot(departure, mix[x * groups + g], preferred_element_type=jnp.float32)
            pool_tmp[s, :, at] = (mixed * scale[x * groups + g]).astype(jnp.bfloat16)
        lanes = pl.ds(pl.multiple_of(x * cols, cols), cols)
        pool_rows[s, :, lanes] = pool_tmp[s, pl.ds(pl.multiple_of(x * half, half), half)]
        copy = remote(
            pool_tmp.at[s, pl.ds(pl.multiple_of(other_x * half, half), half)],
            pool_rows.at[s, :, lanes],
            {"tp": other_x},
        )
        copy.start()
        pool_copies.append(copy)

    arrive(out_x)
    start(out_xy)
    start(out_xs)
    arrive(out_y)
    start(out_ys)
    arrive(own_copies)

    me = x * z_count + z
    source_count = 2 * z_count

    def attn_copy(s, dest_z, dest_x):
        return pltpu.make_async_remote_copy(
            src_ref=attn_own.at[s, pl.ds(dest_z * block + dest_x * half, half)],
            dst_ref=attn_rows.at[
                s, :, pl.ds(pl.multiple_of(me * HEAD_DIM, HEAD_DIM), HEAD_DIM)
            ],
            send_sem=attn_send.at[s, dest_z * 2 + dest_x],
            recv_sem=attn_recv.at[s, me],
            device_id={"sp": dest_z, "tp": dest_x},
            device_id_type=MESH,
        )

    def attention_block(s, index):
        low = index * block
        high = low + block
        query = heads[QUERY, s, low:high]
        gate = jnp.transpose(
            jnp.broadcast_to(gates[s, pl.ds(z, 1), low:high], (HEAD_DIM, block))
        )[:, :1]
        gate = gate * log2_e

        def scored(first, last):
            scores = lax.dot_general(
                query,
                heads[KEY, s, first:last],
                (((1,), (1,)), ((), ())),
                preferred_element_type=jnp.float32,
            )
            row = gates[s, pl.ds(z, 1), first:last] * log2_e
            return scores * (HEAD_DIM ** (-0.5) * log2_e) + (gate - row)

        def weighted(scores, top, first, last):
            lifted = jnp.exp2(scores - top)
            return jnp.sum(lifted, axis=1, keepdims=True), jnp.dot(
                lifted.astype(jnp.bfloat16),
                heads[VALUE, s, first:last],
                preferred_element_type=jnp.float32,
            )

        newest = scored(low, high)
        below = lax.broadcasted_iota(jnp.int32, newest.shape, 1) <= lax.broadcasted_iota(
            jnp.int32, newest.shape, 0
        )
        newest = jnp.where(below, newest, masked_score)
        top = jnp.max(newest, axis=1, keepdims=True)
        if low > 0:
            before = scored(0, low)
            top = jnp.maximum(top, jnp.max(before, axis=1, keepdims=True))
        denominator, total = weighted(newest, top, low, high)
        if low > 0:
            more_sum, more_total = weighted(before, top, 0, low)
            denominator = denominator + more_sum
            total = total + more_total
        attn_own[s, low:high] = (total / denominator).astype(jnp.bfloat16)

    def attention_step(s, carry):
        for index in range(z_count):
            attention_block(s, index)
            for dest_x in range(2):
                here = (z == index) & (x == dest_x)

                @pl.when(jnp.logical_not(here))
                def send(index=index, dest_x=dest_x):
                    attn_copy(s, index, dest_x).start()

                @pl.when(here)
                def keep(index=index, dest_x=dest_x):
                    first = index * block + dest_x * half
                    attn_rows[
                        s, :, pl.ds(pl.multiple_of(me * HEAD_DIM, HEAD_DIM), HEAD_DIM)
                    ] = attn_own[s, first : first + half]

        return carry

    for s in range(seqs):
        arrive(other_copies[s])
        attention_step(s, 0)

    arrive(out_xs)
    arrive(out_ys)
    arrive(out_sib)
    arrive(out_xy)
    start(out_xys)
    for copy in out_local:
        copy.wait()
    arrive(out_xys)

    def out_copy(s):
        return pltpu.make_async_copy(out_stage.at[s], out.at[s], local_sem.at[s])

    tile = min(512, width)

    def output_step(s, carry):
        for by in range(1, source_count):
            source = lax.rem(me + by, source_count)
            pltpu.make_async_copy(
                attn_rows.at[s, :, 0:HEAD_DIM],
                attn_rows.at[s, :, 0:HEAD_DIM],
                attn_recv.at[s, source],
            ).wait()

        def tile_step(n, inner):
            lanes = pl.ds(pl.multiple_of(n * tile, tile), tile)
            result = jnp.dot(
                pool_rows[s], w_out[0, :, lanes], preferred_element_type=jnp.float32
            ) + jnp.dot(attn_rows[s], w_out[1, :, lanes], preferred_element_type=jnp.float32)
            out_stage[s, :, lanes] = result.astype(jnp.bfloat16)
            return inner

        lax.fori_loop(0, width // tile, tile_step, 0)
        out_copy(s).start()
        return carry

    arrive(pool_copies)
    lax.fori_loop(0, seqs, output_step, 0)

    for group in (
        tok_x, in_y, in_sib, in_corner, out_x, out_y, out_sib, out_xy, out_xs, out_ys, out_xys,
        own_copies, *other_copies, pool_copies,
    ):
        for copy in group:
            copy.wait_send()

    @pl.when(z < z_count - 1)
    def border_sent():
        border.wait_send()

    for s in range(seqs):
        for dest_z in range(z_count):
            for dest_x in range(2):

                @pl.when(jnp.logical_not((z == dest_z) & (x == dest_x)))
                def sent(s=s, dest_z=dest_z, dest_x=dest_x):
                    attn_copy(s, dest_z, dest_x).wait_send()

        out_copy(s).wait()


def fast_device(
    tokens,
    norm_gain,
    w_pool_in,
    pool_mix,
    pool_scale,
    w_query,
    w_key,
    w_value,
    gate_cache,
    w_out_pool,
    w_out_attn,
):
    seqs, half, width = tokens.shape
    block = 2 * half
    cols = w_key.shape[1]
    z_count = lax.axis_size("sp")
    length = block * z_count
    edge = 16
    bf16 = jnp.bfloat16
    anywhere = pl.BlockSpec(memory_space=pl.ANY)
    inside = pl.BlockSpec(memory_space=pltpu.VMEM)
    dma = pltpu.SemaphoreType.DMA
    return pl.pallas_call(
        layer_kernel,
        in_specs=[
            anywhere,
            inside,
            anywhere,
            inside,
            inside,
            anywhere,
            anywhere,
            anywhere,
            inside,
            anywhere,
            anywhere,
        ],
        out_specs=anywhere,
        out_shape=jax.ShapeDtypeStruct(tokens.shape, bf16),
        scratch_shapes=[
            pltpu.VMEM((4, width, cols), bf16),
            pltpu.VMEM((2, 2 * cols, width), bf16),
            pltpu.VMEM((seqs, 2, half, width), bf16),
            pltpu.VMEM((2, 3, seqs, z_count, half, HEAD_DIM), bf16),
            pltpu.VMEM((3, seqs, length, HEAD_DIM), bf16),
            pltpu.VMEM((seqs, edge + block, cols), jnp.float32),
            pltpu.VMEM((seqs, edge, cols), bf16),
            pltpu.VMEM((seqs, edge, cols), bf16),
            pltpu.VMEM((seqs, block, cols), bf16),
            pltpu.VMEM((seqs, half, 2 * cols), bf16),
            pltpu.VMEM((seqs, length, HEAD_DIM), bf16),
            pltpu.VMEM((seqs, half, 2 * cols), bf16),
            pltpu.VMEM((seqs, half, width), bf16),
            dma((16,)),
            dma((96,)),
            dma((96,)),
            dma((seqs, 2 * z_count)),
            dma((seqs, 2 * z_count)),
        ],
        compiler_params=pltpu.CompilerParams(
            collective_id=0,
            has_side_effects=True,
            vmem_limit_bytes=60 * 1024 * 1024,
        ),
    )(
        tokens,
        norm_gain.reshape(1, width),
        w_pool_in,
        pool_mix,
        pool_scale.reshape(-1, 1, GROUP_WIDTH),
        w_query,
        w_key,
        w_value,
        gate_cache,
        w_out_pool,
        w_out_attn,
    )


def on_device(*args):
    cols = args[5].shape[1]
    half = args[0].shape[1]
    sp_count = lax.axis_size("sp")
    suited = (
        lax.axis_size("tp") == 2
        and lax.axis_size("fs") == 4
        and cols == sp_count * HEAD_DIM
        and args[2].shape[1] == cols == 4 * GROUP_WIDTH
        and half % 128 == 0
        and args[0].shape[2] == 4 * cols
        and half * 2 * sp_count <= 2048
        and args[0].shape[0] <= 2
    )
    if suited:
        return fast_device(*args)
    return general_device(*args)


def solution(mesh):
    placed = (
        P("fs", ("sp", "tp"), None),
        P(),
        P("fs", "tp"),
        P(),
        P(),
        P("fs", "tp"),
        P("fs", "tp"),
        P("fs", "tp"),
        P("fs", "tp", None),
        P("tp", "fs"),
        P("tp", "fs"),
    )
    return jax.shard_map(
        on_device,
        mesh=mesh,
        in_specs=placed,
        out_specs=P("fs", ("sp", "tp"), None),
        check_vma=False,
    )
```

```python
import jax
import jax.numpy as jnp
from jax import lax
from jax.experimental import pallas as pl
from jax.experimental.pallas import tpu as pltpu
from jax.sharding import PartitionSpec as P

HEAD_DIM = 128
GROUP_WIDTH = 128


norm_eps = 1e-06
widest = 16
masked_score = -1e30


def shifted(x, axis, by):
    length = lax.axis_size(axis)
    pairs = [(i, i + by) for i in range(length) if 0 <= i + by < length]
    return lax.ppermute(x, axis, pairs)


def window_sums(extended):
    outcome = []
    current = extended
    offset = 1
    for doubling in range(4):
        padding = jnp.zeros((offset, extended.shape[1]), jnp.float32)
        current = current + jnp.concatenate([padding, current[:-offset]], axis=0)
        offset = offset * 2
        outcome.append(current[widest - 1 :])
    return outcome


def pool_branch(projected, border, first_group, first_position, mixing, scaling):
    row_count = projected.shape[0]
    channels = projected.shape[1]
    widened = projected.astype(jnp.float32)
    totals = window_sums(jnp.concatenate([border.astype(jnp.float32), widened], axis=0))
    token_positions = first_position + jnp.arange(row_count)
    window_index = (first_group + jnp.arange(channels) // GROUP_WIDTH) % 4
    averaged = jnp.zeros((row_count, channels), jnp.float32)
    for doubling in range(4):
        counted = jnp.minimum(token_positions + 1, 2 ** (doubling + 1)).astype(jnp.float32)
        picked = (window_index == doubling).astype(jnp.float32)
        averaged = averaged + picked[None, :] * totals[doubling] / counted[:, None]
    departure = (averaged - widened).astype(jnp.bfloat16)
    group_count = channels // GROUP_WIDTH
    mixed_rows = jnp.einsum(
        "tgc,gcd->tgd",
        departure.reshape(row_count, group_count, GROUP_WIDTH),
        mixing,
        preferred_element_type=jnp.float32,
    )
    return (mixed_rows.reshape(row_count, channels) * scaling[None, :]).astype(jnp.bfloat16)


def general_device(
    tokens,
    norm_gain,
    w_pool_in,
    pool_mix,
    pool_scale,
    w_query,
    w_key,
    w_value,
    gate_cache,
    w_out_pool,
    w_out_attn,
):
    tp_index = lax.axis_index("tp")
    tp_count = lax.axis_size("tp")
    seq_count = tokens.shape[0]
    own_count = tokens.shape[1]
    token_count = own_count * tp_count
    first_position = lax.axis_index("sp") * token_count
    own_rows = tokens.astype(jnp.float32)
    normed = (
        own_rows
        * lax.rsqrt(jnp.mean(own_rows * own_rows, axis=-1, keepdims=True) + norm_eps)
        * norm_gain[None, None, :]
    ).astype(jnp.bfloat16)
    pool_full, query_full, key_full, value_full, out_pool_full, out_attn_full = (
        lax.all_gather(w_pool_in, "fs", axis=0, tiled=True),
        lax.all_gather(w_query, "fs", axis=0, tiled=True),
        lax.all_gather(w_key, "fs", axis=0, tiled=True),
        lax.all_gather(w_value, "fs", axis=0, tiled=True),
        lax.all_gather(w_out_pool, "fs", axis=1, tiled=True),
        lax.all_gather(w_out_attn, "fs", axis=1, tiled=True),
    )
    pool_cols = w_pool_in.shape[1]
    attn_cols = w_query.shape[1]
    shard_rows = lax.all_gather(normed, "tp", axis=1, tiled=True)
    projected = jnp.concatenate(
        [
            jnp.dot(shard_rows, pool_full, preferred_element_type=jnp.float32).astype(jnp.bfloat16),
            jnp.dot(shard_rows, query_full, preferred_element_type=jnp.float32).astype(
                jnp.bfloat16
            ),
            jnp.dot(shard_rows, key_full, preferred_element_type=jnp.float32).astype(jnp.bfloat16),
            jnp.dot(shard_rows, value_full, preferred_element_type=jnp.float32).astype(
                jnp.bfloat16
            ),
        ],
        axis=2,
    )
    pool_in = projected[:, :, :pool_cols]
    query_proj = projected[:, :, pool_cols : pool_cols + attn_cols]
    key_proj = projected[:, :, pool_cols + attn_cols : pool_cols + 2 * attn_cols]
    value_proj = projected[:, :, pool_cols + 2 * attn_cols :]
    group_local = pool_cols // GROUP_WIDTH
    mixing = lax.dynamic_slice_in_dim(pool_mix, tp_index * group_local, group_local, 0)
    scaling = lax.dynamic_slice_in_dim(pool_scale, tp_index * pool_cols, pool_cols, 0)
    borders = shifted(pool_in[:, token_count - (widest - 1) :], "sp", 1)
    pool_out = jnp.stack(
        [
            pool_branch(
                pool_in[member],
                borders[member],
                tp_index * group_local,
                first_position,
                mixing,
                scaling,
            )
            for member in range(seq_count)
        ],
        axis=0,
    )
    head_count = attn_cols // HEAD_DIM
    query_heads = query_proj.reshape(seq_count, token_count, head_count, HEAD_DIM)
    query_gates = jnp.transpose(
        lax.dynamic_slice_in_dim(gate_cache, first_position, token_count, 2), (0, 2, 1)
    )
    query_positions = first_position + jnp.arange(token_count)
    last_position = first_position + token_count - 1
    score_scale = HEAD_DIM ** (-0.5)
    start_state = (
        jnp.full((seq_count, token_count, head_count), masked_score, jnp.float32),
        jnp.zeros((seq_count, token_count, head_count), jnp.float32),
        jnp.zeros((seq_count, token_count, head_count, HEAD_DIM), jnp.float32),
    )
    key_shard = lax.all_gather(key_proj, "sp", axis=1, tiled=True)
    value_shard = lax.all_gather(value_proj, "sp", axis=1, tiled=True)
    key_total = key_shard.shape[1]
    block_rows = 512

    def one_block(block_state, block_index):
        key_start = block_index * block_rows

        def compute(inner_state):
            running_top, running_sum, running_out = inner_state
            key_block = lax.dynamic_slice_in_dim(key_shard, block_index * block_rows, block_rows, 1)
            value_block = lax.dynamic_slice_in_dim(
                value_shard, block_index * block_rows, block_rows, 1
            )
            key_block = key_block.reshape(seq_count, block_rows, head_count, HEAD_DIM)
            value_block = value_block.reshape(seq_count, block_rows, head_count, HEAD_DIM)
            key_gates = lax.dynamic_slice_in_dim(gate_cache, key_start, block_rows, 2)
            scores = (
                jnp.einsum(
                    "sqhd,skhd->sqhk", query_heads, key_block, preferred_element_type=jnp.float32
                )
                * score_scale
            )
            scores = scores + query_gates[:, :, :, None] - key_gates[:, None, :, :]
            allowed = ((key_start + jnp.arange(block_rows))[None, :] <= query_positions[:, None])[
                None, :, None, :
            ]
            scores = jnp.where(allowed, scores, masked_score)
            new_top = jnp.maximum(running_top, jnp.max(scores, axis=3))
            weights = jnp.where(allowed, jnp.exp(scores - new_top[:, :, :, None]), 0.0)
            shrink = jnp.exp(running_top - new_top)
            running_sum = running_sum * shrink + jnp.sum(weights, axis=3)
            running_out = running_out * shrink[:, :, :, None] + jnp.einsum(
                "sqhk,skhd->sqhd",
                weights.astype(jnp.bfloat16),
                value_block,
                preferred_element_type=jnp.float32,
            )
            return (new_top, running_sum, running_out)

        def unchanged(inner_state):
            return inner_state

        return (lax.cond(key_start <= last_position, compute, unchanged, block_state), None)

    result, unused = lax.scan(one_block, start_state, jnp.arange(key_total // block_rows))
    final_top, final_sum, final_out = result
    attn_out = (
        (final_out / final_sum[:, :, :, None])
        .astype(jnp.bfloat16)
        .reshape(seq_count, token_count, attn_cols)
    )
    pool_flat = jnp.transpose(
        pool_out.reshape(seq_count, tp_count, own_count, pool_cols), (1, 0, 2, 3)
    ).reshape(tp_count * seq_count * own_count, pool_cols)
    attn_flat = jnp.transpose(
        attn_out.reshape(seq_count, tp_count, own_count, attn_cols), (1, 0, 2, 3)
    ).reshape(tp_count * seq_count * own_count, attn_cols)
    summed = lax.psum_scatter(
        (
            jnp.dot(pool_flat, out_pool_full, preferred_element_type=jnp.float32)
            + jnp.dot(attn_flat, out_attn_full, preferred_element_type=jnp.float32)
        ).astype(jnp.bfloat16),
        "tp",
        scatter_dimension=0,
        tiled=True,
    ).astype(jnp.float32)
    return summed.astype(jnp.bfloat16).reshape(seq_count, own_count, summed.shape[1])


log2_e = 1.4426950408889634
MESH = pl.DeviceIdType.MESH
KEY, VALUE, QUERY, POOL = 0, 1, 2, 3


def layer_kernel(
    tokens,
    gain,
    w_pool,
    mix,
    scale,
    w_query,
    w_key,
    w_value,
    gates,
    w_out_pool,
    w_out_attn,
    out,
    w_in,
    w_out,
    rows_ref,
    heads,
    extended,
    border,
    pool_tmp,
    pool_rows,
    attn_own,
    attn_rows,
    out_stage,
    local_sem,
    send_sem,
    recv_sem,
    z_send,
    z_recv,
    attn_send,
    attn_recv,
):
    z = lax.axis_index("sp")
    f = lax.axis_index("fs")
    x = lax.axis_index("tp")
    seqs, half, width = tokens.shape
    block = 2 * half
    depth, cols = w_key.shape
    other_x = 1 - x
    sibling = f + 1 - 2 * lax.rem(f, 2)
    across = lax.rem(f + 2, 4)
    z_count = heads.shape[2]
    edge = border.shape[1]

    def z_at(by):
        return lax.rem(z + by, z_count)

    barrier = pltpu.get_barrier_semaphore()
    peers = [{"tp": other_x}, {"fs": sibling}, {"fs": across}]
    for by in range(1, z_count):
        peers.append({"sp": z_at(by)})
        peers.append({"sp": z_at(by), "tp": other_x})
    for peer in peers:
        pl.semaphore_signal(barrier, inc=1, device_id=peer, device_id_type=MESH)
    pl.semaphore_wait(barrier, len(peers))

    numbers = iter(range(send_sem.shape[0]))

    def remote(source, target, peer):
        number = next(numbers)
        return pltpu.make_async_remote_copy(
            src_ref=source,
            dst_ref=target,
            send_sem=send_sem.at[number],
            recv_sem=recv_sem.at[number],
            device_id=peer,
            device_id_type=MESH,
        )

    local_numbers = iter(range(local_sem.shape[0]))

    def local(source, target):
        return pltpu.make_async_copy(source, target, local_sem.at[next(local_numbers)])

    def in_slot(piece, owner):
        kind, low, high = piece
        at = pl.multiple_of(owner * depth, depth)
        return w_in.at[kind, pl.ds(at, depth), low:high]

    def out_slot(kind, owner_x, owner_f):
        return w_out.at[
            kind,
            pl.ds(pl.multiple_of(owner_x * cols, cols), cols),
            pl.ds(pl.multiple_of(owner_f * depth, depth), depth),
        ]

    w_own = (w_key, w_value, w_query, w_pool)
    out_own = (w_out_pool, w_out_attn)
    pair = 2 * HEAD_DIM
    pieces = [
        (kind, low, low + pair) for kind in (KEY, VALUE, QUERY) for low in range(0, cols, pair)
    ]
    pieces.append((POOL, 0, cols))

    def own_piece(piece):
        kind, low, high = piece
        return w_own[kind].at[:, low:high]

    tok_x = [remote(tokens.at[s], rows_ref.at[s, 1], {"tp": other_x}) for s in range(seqs)]
    in_y = [remote(own_piece(p), in_slot(p, f), {"fs": across}) for p in pieces]
    in_sib = [remote(own_piece(p), in_slot(p, f), {"fs": sibling}) for p in pieces]
    in_corner = [remote(in_slot(p, across), in_slot(p, across), {"fs": sibling}) for p in pieces]
    out_x = [remote(out_own[k], out_slot(k, x, f), {"tp": other_x}) for k in range(2)]
    out_y = [remote(out_own[k], out_slot(k, x, f), {"fs": across}) for k in range(2)]
    out_sib = [remote(out_own[k], out_slot(k, x, f), {"fs": sibling}) for k in range(2)]

    def forwarded(owner_x, owner_f, peer):
        return [
            remote(out_slot(k, owner_x, owner_f), out_slot(k, owner_x, owner_f), peer)
            for k in range(2)
        ]

    out_xy = forwarded(other_x, f, {"fs": across})
    out_xs = forwarded(other_x, f, {"fs": sibling})
    out_ys = forwarded(x, across, {"fs": sibling})
    out_xys = forwarded(other_x, across, {"fs": sibling})
    tok_local = [local(tokens.at[s], rows_ref.at[s, 0]) for s in range(seqs)]
    in_local = [local(own_piece(p), in_slot(p, f)) for p in pieces]
    out_local = [local(out_own[k], out_slot(k, x, f)) for k in range(2)]

    def start(copies):
        for copy in copies:
            copy.start()

    def arrive(copies):
        for copy in copies:
            copy.wait_recv()

    border_number = next(numbers)
    next(numbers)

    def border_copy(dest_x):
        return pltpu.make_async_remote_copy(
            src_ref=tokens.at[:, half - edge :],
            dst_ref=border,
            send_sem=send_sem.at[border_number + dest_x],
            recv_sem=recv_sem.at[border_number],
            device_id={"sp": z_at(1), "tp": dest_x},
            device_id_type=MESH,
        )

    sends_border = (z < z_count - 1) & (x == 1)

    tok_x[0].start()
    start(in_y)
    start(tok_x[1:])
    start(tok_local)
    for copy, copy_sib in zip(in_local, in_sib):
        copy.start()
        copy_sib.start()

    @pl.when(sends_border)
    def send_border():
        for dest_x in range(2):
            border_copy(dest_x).start()

    start(out_x)
    start(out_y)
    start(out_sib)
    start(out_local)

    def normalized(rows):
        values = rows.astype(jnp.float32)
        mean = jnp.mean(values * values, axis=-1, keepdims=True)
        return (values * lax.rsqrt(mean + norm_eps) * gain[...]).astype(jnp.bfloat16)

    def normalize(s, which):
        step_rows = 64

        def step(i, carry):
            at = pl.ds(pl.multiple_of(i * step_rows, step_rows), step_rows)
            rows_ref[s, which, at] = normalized(rows_ref[s, which, at])
            return carry

        lax.fori_loop(0, half // step_rows, step, 0)

    def project(values, kind, low=0, high=cols):
        return jnp.dot(
            values, w_in[kind, :, low:high], preferred_element_type=jnp.float32
        ).astype(jnp.bfloat16)

    def project_heads(s, which, kind, low, high):
        result = project(rows_ref[s, which], kind, low, high)
        at = span(z, x if which == 0 else other_x)
        for h in range(low // HEAD_DIM, high // HEAD_DIM):
            heads[kind, s, h, at] = result[:, h * HEAD_DIM - low : (h + 1) * HEAD_DIM - low]

    def span(owner_z, owner_x):
        return pl.ds(pl.multiple_of(owner_z * block + owner_x * half, half), half)

    for copy in tok_local:
        copy.wait()
    for s in range(seqs):
        normalize(s, 0)

    def weights_ready(k):
        in_local[k].wait()
        in_sib[k].wait_recv()
        in_y[k].wait_recv()
        in_corner[k].start()
        in_corner[k].wait_recv()

    def z_copy(group, kinds, dest, which, which_seqs, first, last):
        at = span(z, x if which == 0 else other_x)
        view = heads.at[kinds, which_seqs, first:last, at]
        return pltpu.make_async_remote_copy(
            src_ref=view,
            dst_ref=view,
            send_sem=z_send.at[group, dest if last - first == 1 else z_count],
            recv_sem=z_recv.at[group, z if last - first == 1 else z_count],
            device_id={"sp": dest},
            device_id_type=MESH,
        )

    def queries_go(dest):
        return z >= 1 if dest == 0 else z >= z_count // 2

    everything = pl.ds(0, seqs)
    groups_z = []
    for kind in (KEY, VALUE, QUERY):
        groups_z.append((pl.ds(kind, 1), 0, everything))
    for s in range(seqs):
        groups_z.append((pl.ds(KEY, 2), 1, pl.ds(s, 1)))
        groups_z.append((pl.ds(QUERY, 1), 1, pl.ds(s, 1)))
    asks = [g == QUERY or (g > QUERY and (g - QUERY) % 2 == 0) for g in range(len(groups_z))]
    middle = z_count // 2

    def each_send(group, dests, act):
        kinds, which, which_seqs = groups_z[group]
        for dest in dests:
            going = z != dest
            if asks[group]:
                going = going & queries_go(dest)

            @pl.when(going)
            def to(dest=dest):
                act(z_copy(group, kinds, dest, which, which_seqs, dest, dest + 1))

        if not asks[group] and dests[0] >= middle:

            @pl.when(z == 0)
            def to_next():
                act(z_copy(group, kinds, 1, which, which_seqs, middle, z_count))

    def each_recv(group):
        kinds, which, which_seqs = groups_z[group]
        for source in range(z_count):
            coming = z != source
            if asks[group]:
                coming = coming & ((z == 0) if source == 1 else (source >= middle))

            @pl.when(coming)
            def came(source=source):
                view = heads.at[kinds, which_seqs, 0:1, pl.ds(0, half)]
                pltpu.make_async_copy(view, view, z_recv.at[group, source]).wait()

        if not asks[group]:

            @pl.when(z == 1)
            def came_next():
                view = heads.at[kinds, which_seqs, middle:z_count, pl.ds(0, half)]
                pltpu.make_async_copy(view, view, z_recv.at[group, z_count]).wait()

    left_dests = tuple(range(middle))
    right_dests = tuple(range(z_count - 1, middle - 1, -1))

    for number, (kind, low, high) in enumerate(pieces[:-1]):
        weights_ready(number)

        def own_step(s, carry, kind=kind, low=low, high=high):
            project_heads(s, 0, kind, low, high)
            return carry

        lax.fori_loop(0, seqs, own_step, 0)
        each_send(kind, left_dests if low == 0 else right_dests, lambda copy: copy.start())

    for s in range(seqs):
        tok_x[s].wait_recv()
        normalize(s, 1)
        for group, kinds in ((3 + 2 * s, (KEY, VALUE)), (4 + 2 * s, (QUERY,))):

            def other_step(kind, carry, s=s):
                project_heads(s, 1, kind, 0, cols)
                return carry

            lax.fori_loop(kinds[0], kinds[-1] + 1, other_step, 0)
            each_send(group, left_dests, lambda copy: copy.start())
            each_send(group, right_dests, lambda copy: copy.start())

    weights_ready(len(pieces) - 1)
    for s in range(seqs):
        for which, owner in ((0, x), (1, other_x)):
            at = pl.multiple_of(edge + owner * half, edge)
            extended[s, pl.ds(at, half)] = project(rows_ref[s, which], POOL).astype(jnp.float32)

    @pl.when(z > 0)
    def take_border():
        border_copy(0).wait_recv()
        for s in range(seqs):
            values = normalized(border[s])
            extended[s, 0:edge] = project(values, POOL).astype(jnp.float32)

    @pl.when(z == 0)
    def no_border():
        extended[:, 0:edge] = jnp.zeros((seqs, edge, cols), jnp.float32)

    groups = cols // GROUP_WIDTH
    pool_copies = []
    for s in range(seqs):
        seen = (
            z * block + lax.broadcasted_iota(jnp.int32, (block, GROUP_WIDTH), 0) + 1
        ).astype(jnp.float32)
        for g in range(groups):
            at = slice(g * GROUP_WIDTH, (g + 1) * GROUP_WIDTH)
            plain = extended[s, :, at]
            total = plain
            for doubling in range(g + 1):
                total = total + pltpu.roll(total, 2**doubling, 0)
            averaged = total[edge:] / jnp.minimum(seen, float(2 ** (g + 1)))
            departure = (averaged - plain[edge:]).astype(jnp.bfloat16)
            mixed = jnp.dot(departure, mix[x * groups + g], preferred_element_type=jnp.float32)
            pool_tmp[s, :, at] = (mixed * scale[x * groups + g]).astype(jnp.bfloat16)
        lanes = pl.ds(pl.multiple_of(x * cols, cols), cols)
        pool_rows[s, :, lanes] = pool_tmp[s, pl.ds(pl.multiple_of(x * half, half), half)]
        copy = remote(
            pool_tmp.at[s, pl.ds(pl.multiple_of(other_x * half, half), half)],
            pool_rows.at[s, :, lanes],
            {"tp": other_x},
        )
        copy.start()
        pool_copies.append(copy)

    arrive(out_x)
    start(out_xy)
    start(out_xs)
    arrive(out_y)
    start(out_ys)


    def head_lanes(owner_x, head):
        at = pl.multiple_of((owner_x * z_count + head) * HEAD_DIM, HEAD_DIM)
        return pl.ds(at, HEAD_DIM)

    def attn_copy(s, index, head, dest_x):
        first = index * block + dest_x * half
        return pltpu.make_async_remote_copy(
            src_ref=attn_own.at[s, head, first : first + half],
            dst_ref=attn_rows.at[s, :, head_lanes(x, head)],
            send_sem=attn_send.at[s, index, head, dest_x],
            recv_sem=attn_recv.at[s, x * z_count + head],
            device_id={"sp": index, "tp": dest_x},
            device_id_type=MESH,
        )

    def attention_block(s, index, head):
        low = index * block
        high = low + block
        query = heads[QUERY, s, head, low:high]
        gate = jnp.transpose(
            jnp.broadcast_to(gates[s, pl.ds(head, 1), low:high], (HEAD_DIM, block))
        )[:, :1]
        gate = gate * log2_e

        def scored(first, last):
            scores = lax.dot_general(
                query,
                heads[KEY, s, head, first:last],
                (((1,), (1,)), ((), ())),
                preferred_element_type=jnp.float32,
            )
            row = gates[s, pl.ds(head, 1), first:last] * log2_e
            return scores * (HEAD_DIM ** (-0.5) * log2_e) + (gate - row)

        def weighted(scores, top, first, last):
            lifted = jnp.exp2(scores - top)
            return jnp.sum(lifted, axis=1, keepdims=True), jnp.dot(
                lifted.astype(jnp.bfloat16),
                heads[VALUE, s, head, first:last],
                preferred_element_type=jnp.float32,
            )

        newest = scored(low, high)
        below = lax.broadcasted_iota(jnp.int32, newest.shape, 1) <= lax.broadcasted_iota(
            jnp.int32, newest.shape, 0
        )
        newest = jnp.where(below, newest, masked_score)
        top = jnp.max(newest, axis=1, keepdims=True)
        if low > 0:
            before = scored(0, low)
            top = jnp.maximum(top, jnp.max(before, axis=1, keepdims=True))
        denominator, total = weighted(newest, top, low, high)
        if low > 0:
            more_sum, more_total = weighted(before, top, 0, low)
            denominator = denominator + more_sum
            total = total + more_total
        attn_own[s, head, low:high] = (total / denominator).astype(jnp.bfloat16)

    def attention_rows(s, index, first_head, last_head):
        def head_step(head, carry):
            attention_block(s, index, head)
            for dest_x in range(2):
                here = (z == index) & (x == dest_x)

                @pl.when(jnp.logical_not(here))
                def send(dest_x=dest_x):
                    attn_copy(s, index, head, dest_x).start()

                @pl.when(here)
                def keep(dest_x=dest_x):
                    first = index * block + dest_x * half
                    attn_rows[s, :, head_lanes(x, head)] = attn_own[
                        s, head, first : first + half
                    ]

            return carry

        lax.fori_loop(first_head, last_head, head_step, 0)

    def heads_of(index):
        if index == 0:
            return 0, z_count
        if index == 1:
            return z, 1 + (z_count - 1) * z
        return z, z + 1

    for s in range(seqs):

        @pl.when(z == 0)
        def first_rows(s=s):
            attention_rows(s, 0, *heads_of(0))

    for s in range(seqs):
        for group in ((KEY, VALUE, QUERY) if s == 0 else ()) + (3 + 2 * s, 4 + 2 * s):
            each_recv(group)

        @pl.when(z < 2)
        def second_rows(s=s):
            attention_rows(s, 1, *heads_of(1))

        for index in range(2, z_count):
            attention_rows(s, index, *heads_of(index))

    arrive(out_xs)
    arrive(out_ys)
    arrive(out_sib)
    arrive(out_xy)
    start(out_xys)
    for copy in out_local:
        copy.wait()
    arrive(out_xys)

    def out_copy(s):
        return pltpu.make_async_copy(out_stage.at[s], out.at[s], local_sem.at[s])

    tile = min(512, width)

    def output_step(s, carry):
        for source_x in range(2):
            for head in range(z_count):
                made_here = (z == 0) | (z == head) | ((z == 1) & (head > 0))

                @pl.when(jnp.logical_not((x == source_x) & made_here))
                def came(source_x=source_x, head=head):
                    view = attn_rows.at[s, :, 0:HEAD_DIM]
                    number = source_x * z_count + head
                    pltpu.make_async_copy(view, view, attn_recv.at[s, number]).wait()

        def tile_step(n, inner):
            lanes = pl.ds(pl.multiple_of(n * tile, tile), tile)
            result = jnp.dot(
                pool_rows[s], w_out[0, :, lanes], preferred_element_type=jnp.float32
            ) + jnp.dot(attn_rows[s], w_out[1, :, lanes], preferred_element_type=jnp.float32)
            out_stage[s, :, lanes] = result.astype(jnp.bfloat16)
            return inner

        lax.fori_loop(0, width // tile, tile_step, 0)
        out_copy(s).start()
        return carry

    arrive(pool_copies)
    lax.fori_loop(0, seqs, output_step, 0)

    for group in (
        tok_x, in_y, in_sib, in_corner, out_x, out_y, out_sib, out_xy, out_xs, out_ys, out_xys,
        pool_copies,
    ):
        for copy in group:
            copy.wait_send()

    @pl.when(sends_border)
    def border_sent():
        for dest_x in range(2):
            border_copy(dest_x).wait_send()

    for group in range(len(groups_z)):
        each_send(group, left_dests, lambda copy: copy.wait_send())
        each_send(group, right_dests, lambda copy: copy.wait_send())

    def attention_sent(s, index):
        def head_step(head, carry):
            for dest_x in range(2):

                @pl.when(jnp.logical_not((z == index) & (x == dest_x)))
                def sent(dest_x=dest_x):
                    attn_copy(s, index, head, dest_x).wait_send()

            return carry

        lax.fori_loop(*heads_of(index), head_step, 0)

    for s in range(seqs):
        pl.when(z == 0)(lambda s=s: attention_sent(s, 0))
        pl.when(z < 2)(lambda s=s: attention_sent(s, 1))
        for index in range(2, z_count):
            attention_sent(s, index)
        out_copy(s).wait()


def fast_device(
    tokens,
    norm_gain,
    w_pool_in,
    pool_mix,
    pool_scale,
    w_query,
    w_key,
    w_value,
    gate_cache,
    w_out_pool,
    w_out_attn,
):
    seqs, half, width = tokens.shape
    block = 2 * half
    cols = w_key.shape[1]
    z_count = lax.axis_size("sp")
    length = block * z_count
    edge = 16
    bf16 = jnp.bfloat16
    anywhere = pl.BlockSpec(memory_space=pl.ANY)
    inside = pl.BlockSpec(memory_space=pltpu.VMEM)
    dma = pltpu.SemaphoreType.DMA
    return pl.pallas_call(
        layer_kernel,
        in_specs=[
            anywhere,
            inside,
            anywhere,
            inside,
            inside,
            anywhere,
            anywhere,
            anywhere,
            inside,
            anywhere,
            anywhere,
        ],
        out_specs=anywhere,
        out_shape=jax.ShapeDtypeStruct(tokens.shape, bf16),
        scratch_shapes=[
            pltpu.VMEM((4, width, cols), bf16),
            pltpu.VMEM((2, 2 * cols, width), bf16),
            pltpu.VMEM((seqs, 2, half, width), bf16),
            pltpu.VMEM((3, seqs, z_count, length, HEAD_DIM), bf16),
            pltpu.VMEM((seqs, edge + block, cols), jnp.float32),
            pltpu.VMEM((seqs, edge, width), bf16),
            pltpu.VMEM((seqs, block, cols), bf16),
            pltpu.VMEM((seqs, half, 2 * cols), bf16),
            pltpu.VMEM((seqs, z_count, length, HEAD_DIM), bf16),
            pltpu.VMEM((seqs, half, 2 * cols), bf16),
            pltpu.VMEM((seqs, half, width), bf16),
            dma((16,)),
            dma((64,)),
            dma((64,)),
            dma((3 + 2 * seqs, z_count + 1)),
            dma((3 + 2 * seqs, z_count + 1)),
            dma((seqs, z_count, z_count, 2)),
            dma((seqs, 2 * z_count)),
        ],
        compiler_params=pltpu.CompilerParams(
            collective_id=0,
            has_side_effects=True,
            vmem_limit_bytes=60 * 1024 * 1024,
        ),
    )(
        tokens,
        norm_gain.reshape(1, width),
        w_pool_in,
        pool_mix,
        pool_scale.reshape(-1, 1, GROUP_WIDTH),
        w_query,
        w_key,
        w_value,
        gate_cache,
        w_out_pool,
        w_out_attn,
    )


def on_device(*args):
    cols = args[5].shape[1]
    half = args[0].shape[1]
    sp_count = lax.axis_size("sp")
    suited = (
        lax.axis_size("tp") == 2
        and lax.axis_size("fs") == 4
        and cols == sp_count * HEAD_DIM
        and args[2].shape[1] == cols == 4 * GROUP_WIDTH
        and half % 128 == 0
        and args[0].shape[2] == 4 * cols
        and half * 2 * sp_count <= 2048
        and sp_count == 4
        and args[0].shape[0] <= 2
    )
    if suited:
        return fast_device(*args)
    return general_device(*args)


def solution(mesh):
    placed = (
        P("fs", ("sp", "tp"), None),
        P(),
        P("fs", "tp"),
        P(),
        P(),
        P("fs", "tp"),
        P("fs", "tp"),
        P("fs", "tp"),
        P("fs", "tp", None),
        P("tp", "fs"),
        P("tp", "fs"),
    )
    return jax.shard_map(
        on_device,
        mesh=mesh,
        in_specs=placed,
        out_specs=P("fs", ("sp", "tp"), None),
        check_vma=False,
    )
```

```python
import jax
import jax.numpy as jnp
from jax import lax
from jax.experimental import pallas as pl
from jax.experimental.pallas import tpu as pltpu
from jax.sharding import PartitionSpec as P

HEAD_DIM = 128
GROUP_WIDTH = 128


norm_eps = 1e-06
widest = 16
masked_score = -1e30


def shifted(x, axis, by):
    length = lax.axis_size(axis)
    pairs = [(i, i + by) for i in range(length) if 0 <= i + by < length]
    return lax.ppermute(x, axis, pairs)


def window_sums(extended):
    outcome = []
    current = extended
    offset = 1
    for doubling in range(4):
        padding = jnp.zeros((offset, extended.shape[1]), jnp.float32)
        current = current + jnp.concatenate([padding, current[:-offset]], axis=0)
        offset = offset * 2
        outcome.append(current[widest - 1 :])
    return outcome


def pool_branch(projected, border, first_group, first_position, mixing, scaling):
    row_count = projected.shape[0]
    channels = projected.shape[1]
    widened = projected.astype(jnp.float32)
    totals = window_sums(jnp.concatenate([border.astype(jnp.float32), widened], axis=0))
    token_positions = first_position + jnp.arange(row_count)
    window_index = (first_group + jnp.arange(channels) // GROUP_WIDTH) % 4
    averaged = jnp.zeros((row_count, channels), jnp.float32)
    for doubling in range(4):
        counted = jnp.minimum(token_positions + 1, 2 ** (doubling + 1)).astype(jnp.float32)
        picked = (window_index == doubling).astype(jnp.float32)
        averaged = averaged + picked[None, :] * totals[doubling] / counted[:, None]
    departure = (averaged - widened).astype(jnp.bfloat16)
    group_count = channels // GROUP_WIDTH
    mixed_rows = jnp.einsum(
        "tgc,gcd->tgd",
        departure.reshape(row_count, group_count, GROUP_WIDTH),
        mixing,
        preferred_element_type=jnp.float32,
    )
    return (mixed_rows.reshape(row_count, channels) * scaling[None, :]).astype(jnp.bfloat16)


def general_device(
    tokens,
    norm_gain,
    w_pool_in,
    pool_mix,
    pool_scale,
    w_query,
    w_key,
    w_value,
    gate_cache,
    w_out_pool,
    w_out_attn,
):
    tp_index = lax.axis_index("tp")
    tp_count = lax.axis_size("tp")
    seq_count = tokens.shape[0]
    own_count = tokens.shape[1]
    token_count = own_count * tp_count
    first_position = lax.axis_index("sp") * token_count
    own_rows = tokens.astype(jnp.float32)
    normed = (
        own_rows
        * lax.rsqrt(jnp.mean(own_rows * own_rows, axis=-1, keepdims=True) + norm_eps)
        * norm_gain[None, None, :]
    ).astype(jnp.bfloat16)
    pool_full, query_full, key_full, value_full, out_pool_full, out_attn_full = (
        lax.all_gather(w_pool_in, "fs", axis=0, tiled=True),
        lax.all_gather(w_query, "fs", axis=0, tiled=True),
        lax.all_gather(w_key, "fs", axis=0, tiled=True),
        lax.all_gather(w_value, "fs", axis=0, tiled=True),
        lax.all_gather(w_out_pool, "fs", axis=1, tiled=True),
        lax.all_gather(w_out_attn, "fs", axis=1, tiled=True),
    )
    pool_cols = w_pool_in.shape[1]
    attn_cols = w_query.shape[1]
    shard_rows = lax.all_gather(normed, "tp", axis=1, tiled=True)
    projected = jnp.concatenate(
        [
            jnp.dot(shard_rows, pool_full, preferred_element_type=jnp.float32).astype(jnp.bfloat16),
            jnp.dot(shard_rows, query_full, preferred_element_type=jnp.float32).astype(
                jnp.bfloat16
            ),
            jnp.dot(shard_rows, key_full, preferred_element_type=jnp.float32).astype(jnp.bfloat16),
            jnp.dot(shard_rows, value_full, preferred_element_type=jnp.float32).astype(
                jnp.bfloat16
            ),
        ],
        axis=2,
    )
    pool_in = projected[:, :, :pool_cols]
    query_proj = projected[:, :, pool_cols : pool_cols + attn_cols]
    key_proj = projected[:, :, pool_cols + attn_cols : pool_cols + 2 * attn_cols]
    value_proj = projected[:, :, pool_cols + 2 * attn_cols :]
    group_local = pool_cols // GROUP_WIDTH
    mixing = lax.dynamic_slice_in_dim(pool_mix, tp_index * group_local, group_local, 0)
    scaling = lax.dynamic_slice_in_dim(pool_scale, tp_index * pool_cols, pool_cols, 0)
    borders = shifted(pool_in[:, token_count - (widest - 1) :], "sp", 1)
    pool_out = jnp.stack(
        [
            pool_branch(
                pool_in[member],
                borders[member],
                tp_index * group_local,
                first_position,
                mixing,
                scaling,
            )
            for member in range(seq_count)
        ],
        axis=0,
    )
    head_count = attn_cols // HEAD_DIM
    query_heads = query_proj.reshape(seq_count, token_count, head_count, HEAD_DIM)
    query_gates = jnp.transpose(
        lax.dynamic_slice_in_dim(gate_cache, first_position, token_count, 2), (0, 2, 1)
    )
    query_positions = first_position + jnp.arange(token_count)
    last_position = first_position + token_count - 1
    score_scale = HEAD_DIM ** (-0.5)
    start_state = (
        jnp.full((seq_count, token_count, head_count), masked_score, jnp.float32),
        jnp.zeros((seq_count, token_count, head_count), jnp.float32),
        jnp.zeros((seq_count, token_count, head_count, HEAD_DIM), jnp.float32),
    )
    key_shard = lax.all_gather(key_proj, "sp", axis=1, tiled=True)
    value_shard = lax.all_gather(value_proj, "sp", axis=1, tiled=True)
    key_total = key_shard.shape[1]
    block_rows = 512

    def one_block(block_state, block_index):
        key_start = block_index * block_rows

        def compute(inner_state):
            running_top, running_sum, running_out = inner_state
            key_block = lax.dynamic_slice_in_dim(key_shard, block_index * block_rows, block_rows, 1)
            value_block = lax.dynamic_slice_in_dim(
                value_shard, block_index * block_rows, block_rows, 1
            )
            key_block = key_block.reshape(seq_count, block_rows, head_count, HEAD_DIM)
            value_block = value_block.reshape(seq_count, block_rows, head_count, HEAD_DIM)
            key_gates = lax.dynamic_slice_in_dim(gate_cache, key_start, block_rows, 2)
            scores = (
                jnp.einsum(
                    "sqhd,skhd->sqhk", query_heads, key_block, preferred_element_type=jnp.float32
                )
                * score_scale
            )
            scores = scores + query_gates[:, :, :, None] - key_gates[:, None, :, :]
            allowed = ((key_start + jnp.arange(block_rows))[None, :] <= query_positions[:, None])[
                None, :, None, :
            ]
            scores = jnp.where(allowed, scores, masked_score)
            new_top = jnp.maximum(running_top, jnp.max(scores, axis=3))
            weights = jnp.where(allowed, jnp.exp(scores - new_top[:, :, :, None]), 0.0)
            shrink = jnp.exp(running_top - new_top)
            running_sum = running_sum * shrink + jnp.sum(weights, axis=3)
            running_out = running_out * shrink[:, :, :, None] + jnp.einsum(
                "sqhk,skhd->sqhd",
                weights.astype(jnp.bfloat16),
                value_block,
                preferred_element_type=jnp.float32,
            )
            return (new_top, running_sum, running_out)

        def unchanged(inner_state):
            return inner_state

        return (lax.cond(key_start <= last_position, compute, unchanged, block_state), None)

    result, unused = lax.scan(one_block, start_state, jnp.arange(key_total // block_rows))
    final_top, final_sum, final_out = result
    attn_out = (
        (final_out / final_sum[:, :, :, None])
        .astype(jnp.bfloat16)
        .reshape(seq_count, token_count, attn_cols)
    )
    pool_flat = jnp.transpose(
        pool_out.reshape(seq_count, tp_count, own_count, pool_cols), (1, 0, 2, 3)
    ).reshape(tp_count * seq_count * own_count, pool_cols)
    attn_flat = jnp.transpose(
        attn_out.reshape(seq_count, tp_count, own_count, attn_cols), (1, 0, 2, 3)
    ).reshape(tp_count * seq_count * own_count, attn_cols)
    summed = lax.psum_scatter(
        (
            jnp.dot(pool_flat, out_pool_full, preferred_element_type=jnp.float32)
            + jnp.dot(attn_flat, out_attn_full, preferred_element_type=jnp.float32)
        ).astype(jnp.bfloat16),
        "tp",
        scatter_dimension=0,
        tiled=True,
    ).astype(jnp.float32)
    return summed.astype(jnp.bfloat16).reshape(seq_count, own_count, summed.shape[1])


log2_e = 1.4426950408889634
MESH = pl.DeviceIdType.MESH
KEY, VALUE, QUERY, POOL = 0, 1, 2, 3


def layer_kernel(
    tokens,
    gain_in,
    w_pool,
    mix_in,
    scale_in,
    w_query,
    w_key,
    w_value,
    gates_in,
    w_out_pool,
    w_out_attn,
    out,
    gain,
    mix,
    scale,
    gates,
    w_in,
    w_out,
    rows_ref,
    heads,
    extended,
    border,
    pool_tmp,
    pool_rows,
    attn_own,
    attn_rows,
    pooled,
    local_sem,
    send_sem,
    recv_sem,
    z_send,
    z_recv,
    attn_send,
    attn_recv,
    border_sem,
    pass_send,
):
    z = lax.axis_index("sp")
    f = lax.axis_index("fs")
    x = lax.axis_index("tp")
    seqs, half, width = tokens.shape
    block = 2 * half
    depth, cols = w_key.shape
    other_x = 1 - x
    sibling = f + 1 - 2 * lax.rem(f, 2)
    across = lax.rem(f + 2, 4)
    z_count = heads.shape[2]
    edge = border.shape[1]

    def z_at(by):
        return lax.rem(z + by, z_count)

    barrier = pltpu.get_barrier_semaphore()
    peers = [{"tp": other_x}, {"fs": sibling}, {"fs": across}]
    for by in range(1, z_count):
        peers.append({"sp": z_at(by)})
        peers.append({"sp": z_at(by), "tp": other_x})
    for peer in peers:
        pl.semaphore_signal(barrier, inc=1, device_id=peer, device_id_type=MESH)
    pl.semaphore_wait(barrier, len(peers))

    numbers = iter(range(send_sem.shape[0]))

    def remote(source, target, peer):
        number = next(numbers)
        return pltpu.make_async_remote_copy(
            src_ref=source,
            dst_ref=target,
            send_sem=send_sem.at[number],
            recv_sem=recv_sem.at[number],
            device_id=peer,
            device_id_type=MESH,
        )

    local_numbers = iter(range(local_sem.shape[0]))

    def local(source, target):
        return pltpu.make_async_copy(source, target, local_sem.at[next(local_numbers)])

    def in_slot(piece, owner):
        kind, low, high = piece
        at = pl.multiple_of(owner * depth, depth)
        return w_in.at[kind, pl.ds(at, depth), low:high]

    def in_part(piece, owner, part):
        kind, low, high = piece
        at = pl.multiple_of(owner * depth + part * (depth // 2), depth // 2)
        return w_in.at[kind, pl.ds(at, depth // 2), low:high]

    def out_slot(kind, owner_x, owner_f):
        return w_out.at[
            kind,
            pl.ds(pl.multiple_of(owner_x * cols, cols), cols),
            pl.ds(pl.multiple_of(owner_f * depth, depth), depth),
        ]

    w_own = (w_key, w_value, w_query, w_pool)
    out_own = (w_out_pool, w_out_attn)
    pair = 2 * HEAD_DIM
    pieces = [
        (kind, low, low + pair) for kind in (KEY, VALUE, QUERY) for low in range(0, cols, pair)
    ]
    pieces.append((POOL, 0, cols))

    def own_piece(piece):
        kind, low, high = piece
        return w_own[kind].at[:, low:high]

    tok_x = [remote(tokens.at[s], rows_ref.at[s, 1], {"tp": other_x}) for s in range(seqs)]
    parity = lax.rem(z, 2)
    partner = z + 1 - 2 * parity
    shared = [p for p in pieces if p[0] == KEY]
    in_y = []
    in_z = []
    in_corner_other = []
    for p in pieces:
        if p in shared:
            kind, low, high = p
            at = pl.multiple_of(parity * (depth // 2), depth // 2)
            source = w_own[kind].at[pl.ds(at, depth // 2), low:high]
            in_y.append(remote(source, in_part(p, f, parity), {"fs": across}))
            view = in_part(p, across, parity)
            in_z.append(remote(view, view, {"sp": partner}))
            view = in_part(p, across, 1 - parity)
            in_corner_other.append(remote(view, view, {"fs": sibling}))
        else:
            in_y.append(remote(own_piece(p), in_slot(p, f), {"fs": across}))
    in_sib = [remote(own_piece(p), in_slot(p, f), {"fs": sibling}) for p in pieces]
    in_corner = []
    for p in pieces:
        view = in_part(p, across, parity) if p in shared else in_slot(p, across)
        in_corner.append(remote(view, view, {"fs": sibling}))
    out_x = [remote(out_own[k], out_slot(k, x, f), {"tp": other_x}) for k in range(2)]
    out_y = [remote(out_own[k], out_slot(k, x, f), {"fs": across}) for k in range(2)]
    out_sib = [remote(out_own[k], out_slot(k, x, f), {"fs": sibling}) for k in range(2)]

    def forwarded(owner_x, owner_f, peer):
        return [
            remote(out_slot(k, owner_x, owner_f), out_slot(k, owner_x, owner_f), peer)
            for k in range(2)
        ]

    out_xy = forwarded(other_x, f, {"fs": across})
    out_xs = forwarded(other_x, f, {"fs": sibling})
    out_ys = forwarded(x, across, {"fs": sibling})
    out_xys = forwarded(other_x, across, {"fs": sibling})
    small_local = [
        local(gain_in, gain),
        local(mix_in, mix),
        local(scale_in, scale),
        local(gates_in, gates),
    ]
    tok_local = [local(tokens.at[s], rows_ref.at[s, 0]) for s in range(seqs)]
    in_local = [local(own_piece(p), in_slot(p, f)) for p in pieces]
    out_local = [local(out_own[k], out_slot(k, x, f)) for k in range(2)]

    def start(copies):
        for copy in copies:
            copy.start()

    def arrive(copies):
        for copy in copies:
            copy.wait_recv()

    def border_copy(s, which):
        return pltpu.make_async_remote_copy(
            src_ref=rows_ref.at[s, which, half - edge :],
            dst_ref=border.at[s],
            send_sem=border_sem.at[0, s],
            recv_sem=border_sem.at[1, s],
            device_id={"sp": z_at(1)},
            device_id_type=MESH,
        )

    def each_border(s, act):
        for which, owner in ((0, 1), (1, 0)):

            @pl.when((z < z_count - 1) & (x == owner))
            def to_next(which=which):
                act(border_copy(s, which))

    tok_x[0].start()
    start(in_y)
    start(tok_x[1:])
    start(tok_local)
    start(small_local)
    start(in_local)
    start(in_sib[:2])

    start(out_x)
    start(out_y)
    start(out_local)

    def normalized(rows):
        values = rows.astype(jnp.float32)
        mean = jnp.mean(values * values, axis=-1, keepdims=True)
        return (values * lax.rsqrt(mean + norm_eps) * gain[...]).astype(jnp.bfloat16)

    def normalize(s, which):
        step_rows = 64

        def step(i, carry):
            at = pl.ds(pl.multiple_of(i * step_rows, step_rows), step_rows)
            rows_ref[s, which, at] = normalized(rows_ref[s, which, at])
            return carry

        lax.fori_loop(0, half // step_rows, step, 0)

    def project(values, kind, low=0, high=cols):
        return jnp.dot(
            values, w_in[kind, :, low:high], preferred_element_type=jnp.float32
        ).astype(jnp.bfloat16)

    def project_heads(s, which, kind, low, high):
        result = project(rows_ref[s, which], kind, low, high)
        at = span(z, x if which == 0 else other_x)
        for h in range(low // HEAD_DIM, high // HEAD_DIM):
            heads[kind, s, h, at] = result[:, h * HEAD_DIM - low : (h + 1) * HEAD_DIM - low]

    def span(owner_z, owner_x):
        return pl.ds(pl.multiple_of(owner_z * block + owner_x * half, half), half)

    for copy in tok_local + small_local:
        copy.wait()
    for s in range(seqs):
        normalize(s, 0)

    def weights_landed(k):
        in_y[k].wait_recv()
        if k < len(shared):
            in_z[k].start()
        in_corner[k].start()

    def weights_ready(k):
        in_local[k].wait()
        in_sib[k].wait_recv()
        if k < len(shared):
            in_z[k].wait_recv()
            in_corner_other[k].start()
            in_corner_other[k].wait_recv()
        in_corner[k].wait_recv()

    def z_copy(group, kinds, dest, which, which_seqs, first, last):
        at = span(z, x if which == 0 else other_x)
        view = heads.at[kinds, which_seqs, first:last, at]
        return pltpu.make_async_remote_copy(
            src_ref=view,
            dst_ref=view,
            send_sem=z_send.at[group, dest if last - first == 1 else z_count],
            recv_sem=z_recv.at[group, z if last - first == 1 else z_count],
            device_id={"sp": dest},
            device_id_type=MESH,
        )

    def queries_go(dest):
        return z >= 1 if dest == 0 else z >= z_count // 2

    everything = pl.ds(0, seqs)
    groups_z = []
    for kind in (KEY, VALUE, QUERY):
        groups_z.append((pl.ds(kind, 1), 0, everything))
    for s in range(seqs):
        groups_z.append((pl.ds(KEY, 2), 1, pl.ds(s, 1)))
        groups_z.append((pl.ds(QUERY, 1), 1, pl.ds(s, 1)))
    asks = [g == QUERY or (g > QUERY and (g - QUERY) % 2 == 0) for g in range(len(groups_z))]
    middle = z_count // 2

    def each_send(group, dests, act):
        kinds, which, which_seqs = groups_z[group]
        for dest in dests:
            going = z != dest
            if asks[group]:
                going = going & queries_go(dest)
            elif dest >= middle:
                going = going & (z > 0)

            @pl.when(going)
            def to(dest=dest):
                act(z_copy(group, kinds, dest, which, which_seqs, dest, dest + 1))

        if not asks[group] and dests[0] >= middle:

            @pl.when(z == 0)
            def to_next():
                act(z_copy(group, kinds, 1, which, which_seqs, middle, z_count))

    def each_recv(group, sources):
        kinds, which, which_seqs = groups_z[group]
        for source in sources:
            coming = z != source
            if asks[group]:
                coming = coming & ((z == 0) if source == 1 else (source >= middle))

            @pl.when(coming)
            def came(source=source):
                view = heads.at[kinds, which_seqs, 0:1, pl.ds(0, half)]
                pltpu.make_async_copy(view, view, z_recv.at[group, source]).wait()

    def pass_copy(group, dest):
        kinds, which, which_seqs = groups_z[group]
        at = span(0, x if which == 0 else other_x)
        view = heads.at[kinds, which_seqs, dest : dest + 1, at]
        return pltpu.make_async_remote_copy(
            src_ref=view,
            dst_ref=view,
            send_sem=pass_send.at[group, dest - middle],
            recv_sem=z_recv.at[group, 0],
            device_id={"sp": dest},
            device_id_type=MESH,
        )

    def pass_on(group):
        kinds, which, which_seqs = groups_z[group]

        @pl.when(z == 1)
        def from_first():
            view = heads.at[kinds, which_seqs, middle:z_count, pl.ds(0, half)]
            pltpu.make_async_copy(view, view, z_recv.at[group, z_count]).wait()
            for dest in right_dests:
                pass_copy(group, dest).start()

    left_dests = tuple(range(middle))
    right_dests = tuple(range(z_count - 1, middle - 1, -1))

    weights_landed(0)
    for number, (kind, low, high) in enumerate(pieces[:-1]):
        if number + 1 < len(shared):
            weights_landed(number + 1)
        if number + 2 < len(pieces):
            in_sib[number + 2].start()
        if number >= len(shared):
            weights_landed(number)
        weights_ready(number)

        def own_step(s, carry, kind=kind, low=low, high=high):
            project_heads(s, 0, kind, low, high)
            return carry

        lax.fori_loop(0, seqs, own_step, 0)
        each_send(kind, left_dests if low == 0 else right_dests, lambda copy: copy.start())
        if kind > KEY and low > 0:
            pass_on(kind - 1)

    def other_rows(s):
        tok_x[s].wait_recv()
        normalize(s, 1)
        each_border(s, lambda copy: copy.start())
        for group, kinds in ((3 + 2 * s, (KEY, VALUE)), (4 + 2 * s, (QUERY,))):

            def other_step(kind, carry, s=s):
                project_heads(s, 1, kind, 0, cols)
                return carry

            lax.fori_loop(kinds[0], kinds[-1] + 1, other_step, 0)
            each_send(group, left_dests, lambda copy: copy.start())
            each_send(group, right_dests, lambda copy: copy.start())

    @pl.when(z == 0)
    def no_border():
        extended[:, 0:edge] = jnp.zeros((seqs, edge, cols), jnp.float32)

    def take_border(s):
        @pl.when(z > 0)
        def take():
            border_copy(s, 0).wait_recv()
            extended[s, 0:edge] = project(border[s], POOL).astype(jnp.float32)

    groups = cols // GROUP_WIDTH
    own_lanes = pl.ds(pl.multiple_of(x * cols, cols), cols)
    pool_copies = [
        remote(
            pool_tmp.at[s, pl.ds(pl.multiple_of(other_x * half, half), half)],
            pool_rows.at[s, :, own_lanes],
            {"tp": other_x},
        )
        for s in range(seqs)
    ]

    def pool_branch_rows(s):
        for which, owner in ((0, x), (1, other_x)):
            at = pl.multiple_of(edge + owner * half, edge)
            extended[s, pl.ds(at, half)] = project(rows_ref[s, which], POOL).astype(jnp.float32)
        seen = (
            z * block + lax.broadcasted_iota(jnp.int32, (block, GROUP_WIDTH), 0) + 1
        ).astype(jnp.float32)
        for g in range(groups):
            at = slice(g * GROUP_WIDTH, (g + 1) * GROUP_WIDTH)
            plain = extended[s, :, at]
            total = plain
            for doubling in range(g + 1):
                total = total + pltpu.roll(total, 2**doubling, 0)
            averaged = total[edge:] / jnp.minimum(seen, float(2 ** (g + 1)))
            departure = (averaged - plain[edge:]).astype(jnp.bfloat16)
            mixed = jnp.dot(departure, mix[x * groups + g], preferred_element_type=jnp.float32)
            pool_tmp[s, :, at] = (mixed * scale[x * groups + g]).astype(jnp.bfloat16)
        pool_rows[s, :, own_lanes] = pool_tmp[s, pl.ds(pl.multiple_of(x * half, half), half)]
        pool_copies[s].start()

    def head_lanes(owner_x, head):
        at = pl.multiple_of((owner_x * z_count + head) * HEAD_DIM, HEAD_DIM)
        return pl.ds(at, HEAD_DIM)

    def attn_slot(index, head):
        return head if index == 0 else z_count + head if index == 1 else 2 * z_count + index - 2

    def attn_copy(s, index, head, dest_x):
        first = index * block + dest_x * half
        return pltpu.make_async_remote_copy(
            src_ref=attn_own.at[s, head, first : first + half],
            dst_ref=attn_rows.at[s, :, head_lanes(x, head)],
            send_sem=attn_send.at[s, attn_slot(index, head), dest_x],
            recv_sem=attn_recv.at[s, x * z_count + head],
            device_id={"sp": index, "tp": dest_x},
            device_id_type=MESH,
        )

    def attention_block(s, index, head):
        low = index * block
        high = low + block
        query = heads[QUERY, s, head, low:high]
        gate = jnp.transpose(
            jnp.broadcast_to(gates[s, pl.ds(head, 1), low:high], (HEAD_DIM, block))
        )[:, :1]
        gate = gate * log2_e

        def scored(first, last):
            scores = lax.dot_general(
                query,
                heads[KEY, s, head, first:last],
                (((1,), (1,)), ((), ())),
                preferred_element_type=jnp.float32,
            )
            row = gates[s, pl.ds(head, 1), first:last] * log2_e
            return scores * (HEAD_DIM ** (-0.5) * log2_e) + (gate - row)

        def weighted(scores, top, first, last):
            lifted = jnp.exp2(scores - top)
            return jnp.sum(lifted, axis=1, keepdims=True), jnp.dot(
                lifted.astype(jnp.bfloat16),
                heads[VALUE, s, head, first:last],
                preferred_element_type=jnp.float32,
            )

        newest = scored(low, high)
        below = lax.broadcasted_iota(jnp.int32, newest.shape, 1) <= lax.broadcasted_iota(
            jnp.int32, newest.shape, 0
        )
        newest = jnp.where(below, newest, masked_score)
        top = jnp.max(newest, axis=1, keepdims=True)
        if low > 0:
            before = scored(0, low)
            top = jnp.maximum(top, jnp.max(before, axis=1, keepdims=True))
        denominator, total = weighted(newest, top, low, high)
        if low > 0:
            more_sum, more_total = weighted(before, top, 0, low)
            denominator = denominator + more_sum
            total = total + more_total
        attn_own[s, head, low:high] = (total / denominator).astype(jnp.bfloat16)

    def attention_rows(s, index, first_head, last_head):
        def head_step(head, carry):
            attention_block(s, index, head)
            for dest_x in range(2):
                here = (z == index) & (x == dest_x)

                @pl.when(jnp.logical_not(here))
                def send(dest_x=dest_x):
                    attn_copy(s, index, head, dest_x).start()

                @pl.when(here)
                def keep(dest_x=dest_x):
                    first = index * block + dest_x * half
                    attn_rows[s, :, head_lanes(x, head)] = attn_own[
                        s, head, first : first + half
                    ]

            return carry

        lax.fori_loop(first_head, last_head, head_step, 0)

    def heads_of(index):
        if index == 0:
            return 0, z_count
        if index == 1:
            return z, 1 + (z_count - 1) * z
        return z, z + 1

    def first_rows(s):
        pl.when(z == 0)(lambda: attention_rows(s, 0, *heads_of(0)))

    def later_rows(s):
        arriving = ((KEY, VALUE, QUERY) if s == 0 else ()) + (3 + 2 * s, 4 + 2 * s)
        for group in arriving:
            each_recv(group, range(middle))
        pl.when(z < 2)(lambda: attention_rows(s, 1, *heads_of(1)))
        if s == 0:
            forward_half(0)
        for index in range(middle, z_count):
            for group in arriving:
                each_recv(group, (index,))
            attention_rows(s, index, *heads_of(index))

    def forward_half(kind):
        out_x[kind].wait_recv()
        out_xy[kind].start()
        out_xs[kind].start()

    for s in range(seqs):
        other_rows(s)
        if s == 0:
            start(out_sib)
            weights_landed(len(pieces) - 1)
            weights_ready(len(pieces) - 1)
        take_border(s)
        pool_branch_rows(s)
        pass_on(3 + 2 * s)
        first_rows(s)

    for s in range(seqs):
        later_rows(s)
        if s == 0:
            arrive(out_y)
            start(out_ys)
            forward_half(1)

    for group in (tok_x, in_y, in_sib, in_corner, in_z, in_corner_other, out_x, out_y, out_sib):
        for copy in group:
            copy.wait_send()
    for s in range(seqs):
        each_border(s, lambda copy: copy.wait_send())

    for group in range(len(groups_z)):
        if not asks[group]:
            for dest in right_dests:
                pl.when(z == 1)(lambda group=group, dest=dest: pass_copy(group, dest).wait_send())
        each_send(group, left_dests, lambda copy: copy.wait_send())
        each_send(group, right_dests, lambda copy: copy.wait_send())
    for copy in out_local:
        copy.wait()

    arrive(out_xy)
    start(out_xys)
    arrive(out_xs)
    arrive(out_ys)
    arrive(out_sib)
    arrive(pool_copies)

    tiles = [f, sibling, across, f + 2 - 4 * (f // 2) + 1 - 2 * lax.rem(f, 2)]

    def tile_lanes(tile):
        return pl.ds(pl.multiple_of(tile * depth, depth), depth)

    def pool_part(s, tile):
        return jnp.dot(
            pool_rows[s], w_out[0, :, tile_lanes(tile)], preferred_element_type=jnp.float32
        )

    def attn_part(s, tile):
        return jnp.dot(
            attn_rows[s], w_out[1, :, tile_lanes(tile)], preferred_element_type=jnp.float32
        )

    def attention_came(s):
        for source_x in range(2):
            for head in range(z_count):
                made_here = (z == 0) | (z == head) | ((z == 1) & (head > 0))

                @pl.when(jnp.logical_not((x == source_x) & made_here))
                def came(source_x=source_x, head=head):
                    view = attn_rows.at[s, :, 0:HEAD_DIM]
                    number = source_x * z_count + head
                    pltpu.make_async_copy(view, view, attn_recv.at[s, number]).wait()

    for s in range(seqs - 1):
        attention_came(s)
        for number, tile in enumerate(tiles):
            if s == 0 and number == len(tiles) - 1:
                arrive(out_xys)
            result = pool_part(s, tile) + attn_part(s, tile)
            out[s, :, tile_lanes(tile)] = result.astype(jnp.bfloat16)
    last = seqs - 1
    if last == 0:
        arrive(out_xys)
    for tile in tiles:
        pooled[:, tile_lanes(tile)] = pool_part(last, tile)
    attention_came(last)
    for tile in tiles:
        result = pooled[:, tile_lanes(tile)] + attn_part(last, tile)
        out[last, :, tile_lanes(tile)] = result.astype(jnp.bfloat16)

    for group in (
        out_xy, out_xs, out_ys, out_xys,
        pool_copies,
    ):
        for copy in group:
            copy.wait_send()

    def attention_sent(s, index):
        def head_step(head, carry):
            for dest_x in range(2):

                @pl.when(jnp.logical_not((z == index) & (x == dest_x)))
                def sent(dest_x=dest_x):
                    attn_copy(s, index, head, dest_x).wait_send()

            return carry

        lax.fori_loop(*heads_of(index), head_step, 0)

    for s in range(seqs):
        pl.when(z == 0)(lambda s=s: attention_sent(s, 0))
        pl.when(z < 2)(lambda s=s: attention_sent(s, 1))
        for index in range(2, z_count):
            attention_sent(s, index)


def fast_device(
    tokens,
    norm_gain,
    w_pool_in,
    pool_mix,
    pool_scale,
    w_query,
    w_key,
    w_value,
    gate_cache,
    w_out_pool,
    w_out_attn,
):
    seqs, half, width = tokens.shape
    block = 2 * half
    cols = w_key.shape[1]
    z_count = lax.axis_size("sp")
    length = block * z_count
    edge = 16
    bf16 = jnp.bfloat16
    anywhere = pl.BlockSpec(memory_space=pl.ANY)
    inside = pl.BlockSpec(memory_space=pltpu.VMEM)
    dma = pltpu.SemaphoreType.DMA
    return pl.pallas_call(
        layer_kernel,
        in_specs=[anywhere] * 11,
        out_specs=inside,
        out_shape=pltpu.VMEM(tokens.shape, bf16),
        scratch_shapes=[
            pltpu.VMEM((1, width), jnp.float32),
            pltpu.VMEM(pool_mix.shape, bf16),
            pltpu.VMEM((pool_mix.shape[0], 1, GROUP_WIDTH), jnp.float32),
            pltpu.VMEM(gate_cache.shape, jnp.float32),
            pltpu.VMEM((4, width, cols), bf16),
            pltpu.VMEM((2, 2 * cols, width), bf16),
            pltpu.VMEM((seqs, 2, half, width), bf16),
            pltpu.VMEM((3, seqs, z_count, length, HEAD_DIM), bf16),
            pltpu.VMEM((seqs, edge + block, cols), jnp.float32),
            pltpu.VMEM((seqs, edge, width), bf16),
            pltpu.VMEM((seqs, block, cols), bf16),
            pltpu.VMEM((seqs, half, 2 * cols), bf16),
            pltpu.VMEM((seqs, z_count, length, HEAD_DIM), bf16),
            pltpu.VMEM((seqs, half, 2 * cols), bf16),
            pltpu.VMEM((half, width), jnp.float32),
            dma((13 + seqs,)),
            dma((39 + 2 * seqs,)),
            dma((39 + 2 * seqs,)),
            dma((3 + 2 * seqs, z_count + 1)),
            dma((3 + 2 * seqs, z_count + 1)),
            dma((seqs, 2 * z_count + 2, 2)),
            dma((seqs, 2 * z_count)),
            dma((2, seqs)),
            dma((3 + 2 * seqs, z_count // 2)),
        ],
        compiler_params=pltpu.CompilerParams(
            collective_id=0,
            has_side_effects=True,
            vmem_limit_bytes=54 * 1024 * 1024,
        ),
    )(
        tokens,
        norm_gain.reshape(1, width),
        w_pool_in,
        pool_mix,
        pool_scale.reshape(-1, 1, GROUP_WIDTH),
        w_query,
        w_key,
        w_value,
        gate_cache,
        w_out_pool,
        w_out_attn,
    )


def on_device(*args):
    cols = args[5].shape[1]
    half = args[0].shape[1]
    sp_count = lax.axis_size("sp")
    suited = (
        lax.axis_size("tp") == 2
        and lax.axis_size("fs") == 4
        and cols == sp_count * HEAD_DIM
        and args[2].shape[1] == cols == 4 * GROUP_WIDTH
        and half % 128 == 0
        and args[0].shape[2] == 4 * cols
        and half * 2 * sp_count <= 2048
        and sp_count == 4
        and args[0].shape[0] <= 2
    )
    if suited:
        return fast_device(*args)
    return general_device(*args)


def solution(mesh):
    placed = (
        P("fs", ("sp", "tp"), None),
        P(),
        P("fs", "tp"),
        P(),
        P(),
        P("fs", "tp"),
        P("fs", "tp"),
        P("fs", "tp"),
        P("fs", "tp", None),
        P("tp", "fs"),
        P("tp", "fs"),
    )
    return jax.shard_map(
        on_device,
        mesh=mesh,
        in_specs=placed,
        out_specs=P("fs", ("sp", "tp"), None),
        check_vma=False,
    )
```

```python
import jax
import jax.numpy as jnp
from jax import lax
from jax.experimental import pallas as pl
from jax.experimental.pallas import tpu as pltpu
from jax.sharding import PartitionSpec as P

HEAD_DIM = 128
GROUP_WIDTH = 128


norm_eps = 1e-06
widest = 16
masked_score = -1e30


def shifted(x, axis, by):
    length = lax.axis_size(axis)
    pairs = [(i, i + by) for i in range(length) if 0 <= i + by < length]
    return lax.ppermute(x, axis, pairs)


def window_sums(extended):
    outcome = []
    current = extended
    offset = 1
    for doubling in range(4):
        padding = jnp.zeros((offset, extended.shape[1]), jnp.float32)
        current = current + jnp.concatenate([padding, current[:-offset]], axis=0)
        offset = offset * 2
        outcome.append(current[widest - 1 :])
    return outcome


def pool_branch(projected, border, first_group, first_position, mixing, scaling):
    row_count = projected.shape[0]
    channels = projected.shape[1]
    widened = projected.astype(jnp.float32)
    totals = window_sums(jnp.concatenate([border.astype(jnp.float32), widened], axis=0))
    token_positions = first_position + jnp.arange(row_count)
    window_index = (first_group + jnp.arange(channels) // GROUP_WIDTH) % 4
    averaged = jnp.zeros((row_count, channels), jnp.float32)
    for doubling in range(4):
        counted = jnp.minimum(token_positions + 1, 2 ** (doubling + 1)).astype(jnp.float32)
        picked = (window_index == doubling).astype(jnp.float32)
        averaged = averaged + picked[None, :] * totals[doubling] / counted[:, None]
    departure = (averaged - widened).astype(jnp.bfloat16)
    group_count = channels // GROUP_WIDTH
    mixed_rows = jnp.einsum(
        "tgc,gcd->tgd",
        departure.reshape(row_count, group_count, GROUP_WIDTH),
        mixing,
        preferred_element_type=jnp.float32,
    )
    return (mixed_rows.reshape(row_count, channels) * scaling[None, :]).astype(jnp.bfloat16)


def general_device(
    tokens,
    norm_gain,
    w_pool_in,
    pool_mix,
    pool_scale,
    w_query,
    w_key,
    w_value,
    gate_cache,
    w_out_pool,
    w_out_attn,
):
    tp_index = lax.axis_index("tp")
    tp_count = lax.axis_size("tp")
    seq_count = tokens.shape[0]
    own_count = tokens.shape[1]
    token_count = own_count * tp_count
    first_position = lax.axis_index("sp") * token_count
    own_rows = tokens.astype(jnp.float32)
    normed = (
        own_rows
        * lax.rsqrt(jnp.mean(own_rows * own_rows, axis=-1, keepdims=True) + norm_eps)
        * norm_gain[None, None, :]
    ).astype(jnp.bfloat16)
    pool_full, query_full, key_full, value_full, out_pool_full, out_attn_full = (
        lax.all_gather(w_pool_in, "fs", axis=0, tiled=True),
        lax.all_gather(w_query, "fs", axis=0, tiled=True),
        lax.all_gather(w_key, "fs", axis=0, tiled=True),
        lax.all_gather(w_value, "fs", axis=0, tiled=True),
        lax.all_gather(w_out_pool, "fs", axis=1, tiled=True),
        lax.all_gather(w_out_attn, "fs", axis=1, tiled=True),
    )
    pool_cols = w_pool_in.shape[1]
    attn_cols = w_query.shape[1]
    shard_rows = lax.all_gather(normed, "tp", axis=1, tiled=True)
    projected = jnp.concatenate(
        [
            jnp.dot(shard_rows, pool_full, preferred_element_type=jnp.float32).astype(jnp.bfloat16),
            jnp.dot(shard_rows, query_full, preferred_element_type=jnp.float32).astype(
                jnp.bfloat16
            ),
            jnp.dot(shard_rows, key_full, preferred_element_type=jnp.float32).astype(jnp.bfloat16),
            jnp.dot(shard_rows, value_full, preferred_element_type=jnp.float32).astype(
                jnp.bfloat16
            ),
        ],
        axis=2,
    )
    pool_in = projected[:, :, :pool_cols]
    query_proj = projected[:, :, pool_cols : pool_cols + attn_cols]
    key_proj = projected[:, :, pool_cols + attn_cols : pool_cols + 2 * attn_cols]
    value_proj = projected[:, :, pool_cols + 2 * attn_cols :]
    group_local = pool_cols // GROUP_WIDTH
    mixing = lax.dynamic_slice_in_dim(pool_mix, tp_index * group_local, group_local, 0)
    scaling = lax.dynamic_slice_in_dim(pool_scale, tp_index * pool_cols, pool_cols, 0)
    borders = shifted(pool_in[:, token_count - (widest - 1) :], "sp", 1)
    pool_out = jnp.stack(
        [
            pool_branch(
                pool_in[member],
                borders[member],
                tp_index * group_local,
                first_position,
                mixing,
                scaling,
            )
            for member in range(seq_count)
        ],
        axis=0,
    )
    head_count = attn_cols // HEAD_DIM
    query_heads = query_proj.reshape(seq_count, token_count, head_count, HEAD_DIM)
    query_gates = jnp.transpose(
        lax.dynamic_slice_in_dim(gate_cache, first_position, token_count, 2), (0, 2, 1)
    )
    query_positions = first_position + jnp.arange(token_count)
    last_position = first_position + token_count - 1
    score_scale = HEAD_DIM ** (-0.5)
    start_state = (
        jnp.full((seq_count, token_count, head_count), masked_score, jnp.float32),
        jnp.zeros((seq_count, token_count, head_count), jnp.float32),
        jnp.zeros((seq_count, token_count, head_count, HEAD_DIM), jnp.float32),
    )
    key_shard = lax.all_gather(key_proj, "sp", axis=1, tiled=True)
    value_shard = lax.all_gather(value_proj, "sp", axis=1, tiled=True)
    key_total = key_shard.shape[1]
    block_rows = 512

    def one_block(block_state, block_index):
        key_start = block_index * block_rows

        def compute(inner_state):
            running_top, running_sum, running_out = inner_state
            key_block = lax.dynamic_slice_in_dim(key_shard, block_index * block_rows, block_rows, 1)
            value_block = lax.dynamic_slice_in_dim(
                value_shard, block_index * block_rows, block_rows, 1
            )
            key_block = key_block.reshape(seq_count, block_rows, head_count, HEAD_DIM)
            value_block = value_block.reshape(seq_count, block_rows, head_count, HEAD_DIM)
            key_gates = lax.dynamic_slice_in_dim(gate_cache, key_start, block_rows, 2)
            scores = (
                jnp.einsum(
                    "sqhd,skhd->sqhk", query_heads, key_block, preferred_element_type=jnp.float32
                )
                * score_scale
            )
            scores = scores + query_gates[:, :, :, None] - key_gates[:, None, :, :]
            allowed = ((key_start + jnp.arange(block_rows))[None, :] <= query_positions[:, None])[
                None, :, None, :
            ]
            scores = jnp.where(allowed, scores, masked_score)
            new_top = jnp.maximum(running_top, jnp.max(scores, axis=3))
            weights = jnp.where(allowed, jnp.exp(scores - new_top[:, :, :, None]), 0.0)
            shrink = jnp.exp(running_top - new_top)
            running_sum = running_sum * shrink + jnp.sum(weights, axis=3)
            running_out = running_out * shrink[:, :, :, None] + jnp.einsum(
                "sqhk,skhd->sqhd",
                weights.astype(jnp.bfloat16),
                value_block,
                preferred_element_type=jnp.float32,
            )
            return (new_top, running_sum, running_out)

        def unchanged(inner_state):
            return inner_state

        return (lax.cond(key_start <= last_position, compute, unchanged, block_state), None)

    result, unused = lax.scan(one_block, start_state, jnp.arange(key_total // block_rows))
    final_top, final_sum, final_out = result
    attn_out = (
        (final_out / final_sum[:, :, :, None])
        .astype(jnp.bfloat16)
        .reshape(seq_count, token_count, attn_cols)
    )
    pool_flat = jnp.transpose(
        pool_out.reshape(seq_count, tp_count, own_count, pool_cols), (1, 0, 2, 3)
    ).reshape(tp_count * seq_count * own_count, pool_cols)
    attn_flat = jnp.transpose(
        attn_out.reshape(seq_count, tp_count, own_count, attn_cols), (1, 0, 2, 3)
    ).reshape(tp_count * seq_count * own_count, attn_cols)
    summed = lax.psum_scatter(
        (
            jnp.dot(pool_flat, out_pool_full, preferred_element_type=jnp.float32)
            + jnp.dot(attn_flat, out_attn_full, preferred_element_type=jnp.float32)
        ).astype(jnp.bfloat16),
        "tp",
        scatter_dimension=0,
        tiled=True,
    ).astype(jnp.float32)
    return summed.astype(jnp.bfloat16).reshape(seq_count, own_count, summed.shape[1])


log2_e = 1.4426950408889634
MESH = pl.DeviceIdType.MESH
KEY, VALUE, QUERY, POOL = 0, 1, 2, 3


def layer_kernel(
    tokens,
    gain_in,
    w_pool,
    mix_in,
    scale_in,
    w_query,
    w_key,
    w_value,
    gates_in,
    w_out_pool,
    w_out_attn,
    out,
    gain,
    mix,
    scale,
    gates,
    w_in,
    w_out,
    rows_ref,
    heads,
    extended,
    border,
    pool_tmp,
    pool_rows,
    attn_own,
    attn_rows,
    pooled,
    local_sem,
    send_sem,
    recv_sem,
    z_send,
    z_recv,
    attn_send,
    attn_recv,
    border_sem,
    pass_send,
):
    z = lax.axis_index("sp")
    f = lax.axis_index("fs")
    x = lax.axis_index("tp")
    seqs, half, width = tokens.shape
    block = 2 * half
    depth, cols = w_key.shape
    other_x = 1 - x
    sibling = f + 1 - 2 * lax.rem(f, 2)
    across = lax.rem(f + 2, 4)
    z_count = heads.shape[2]
    edge = border.shape[1]

    def z_at(by):
        return lax.rem(z + by, z_count)

    barrier = pltpu.get_barrier_semaphore()
    peers = [{"tp": other_x}, {"fs": sibling}, {"fs": across}]
    for by in range(1, z_count):
        peers.append({"sp": z_at(by)})
        peers.append({"sp": z_at(by), "tp": other_x})
    for peer in peers:
        pl.semaphore_signal(barrier, inc=1, device_id=peer, device_id_type=MESH)
    pl.semaphore_wait(barrier, len(peers))

    numbers = iter(range(send_sem.shape[0]))

    def remote(source, target, peer):
        number = next(numbers)
        return pltpu.make_async_remote_copy(
            src_ref=source,
            dst_ref=target,
            send_sem=send_sem.at[number],
            recv_sem=recv_sem.at[number],
            device_id=peer,
            device_id_type=MESH,
        )

    local_numbers = iter(range(local_sem.shape[0]))

    def local(source, target):
        return pltpu.make_async_copy(source, target, local_sem.at[next(local_numbers)])

    def in_slot(piece, owner):
        kind, low, high = piece
        at = pl.multiple_of(owner * depth, depth)
        return w_in.at[kind, pl.ds(at, depth), low:high]

    def in_part(piece, owner, part):
        kind, low, high = piece
        at = pl.multiple_of(owner * depth + part * (depth // 2), depth // 2)
        return w_in.at[kind, pl.ds(at, depth // 2), low:high]

    def out_slot(kind, owner_x, owner_f):
        return w_out.at[
            kind,
            pl.ds(pl.multiple_of(owner_x * cols, cols), cols),
            pl.ds(pl.multiple_of(owner_f * depth, depth), depth),
        ]

    w_own = (w_key, w_value, w_query, w_pool)
    out_own = (w_out_pool, w_out_attn)
    pair = 2 * HEAD_DIM
    pieces = [
        (kind, low, low + pair) for kind in (KEY, VALUE, QUERY) for low in range(0, cols, pair)
    ]
    pieces.append((POOL, 0, cols))

    def own_piece(piece):
        kind, low, high = piece
        return w_own[kind].at[:, low:high]

    tok_x = [remote(tokens.at[s], rows_ref.at[s, 1], {"tp": other_x}) for s in range(seqs)]
    parity = lax.rem(z, 2)
    partner = z + 1 - 2 * parity
    shared = [p for p in pieces if p[0] == KEY]
    in_y = []
    in_z = []
    in_corner_other = []
    for p in pieces:
        if p in shared:
            kind, low, high = p
            at = pl.multiple_of(parity * (depth // 2), depth // 2)
            source = w_own[kind].at[pl.ds(at, depth // 2), low:high]
            in_y.append(remote(source, in_part(p, f, parity), {"fs": across}))
            view = in_part(p, across, parity)
            in_z.append(remote(view, view, {"sp": partner}))
            view = in_part(p, across, 1 - parity)
            in_corner_other.append(remote(view, view, {"fs": sibling}))
        else:
            in_y.append(remote(own_piece(p), in_slot(p, f), {"fs": across}))
    in_sib = [remote(own_piece(p), in_slot(p, f), {"fs": sibling}) for p in pieces]
    in_corner = []
    for p in pieces:
        view = in_part(p, across, parity) if p in shared else in_slot(p, across)
        in_corner.append(remote(view, view, {"fs": sibling}))
    out_x = [remote(out_own[k], out_slot(k, x, f), {"tp": other_x}) for k in range(2)]
    out_y = [remote(out_own[k], out_slot(k, x, f), {"fs": across}) for k in range(2)]
    out_sib = [remote(out_own[k], out_slot(k, x, f), {"fs": sibling}) for k in range(2)]

    def forwarded(owner_x, owner_f, peer):
        return [
            remote(out_slot(k, owner_x, owner_f), out_slot(k, owner_x, owner_f), peer)
            for k in range(2)
        ]

    out_xy = forwarded(other_x, f, {"fs": across})
    out_xs = forwarded(other_x, f, {"fs": sibling})
    out_ys = forwarded(x, across, {"fs": sibling})
    out_xys = forwarded(other_x, across, {"fs": sibling})
    small_local = [
        local(gain_in, gain),
        local(mix_in, mix),
        local(scale_in, scale),
        local(gates_in, gates),
    ]
    tok_local = [local(tokens.at[s], rows_ref.at[s, 0]) for s in range(seqs)]
    in_local = [local(own_piece(p), in_slot(p, f)) for p in pieces]
    out_local = [local(out_own[k], out_slot(k, x, f)) for k in range(2)]

    def start(copies):
        for copy in copies:
            copy.start()

    def arrive(copies):
        for copy in copies:
            copy.wait_recv()

    def border_copy(s, which):
        return pltpu.make_async_remote_copy(
            src_ref=rows_ref.at[s, which, half - edge :],
            dst_ref=border.at[s],
            send_sem=border_sem.at[0, s],
            recv_sem=border_sem.at[1, s],
            device_id={"sp": z_at(1)},
            device_id_type=MESH,
        )

    def each_border(s, act):
        for which, owner in ((0, 1), (1, 0)):

            @pl.when((z < z_count - 1) & (x == owner))
            def to_next(which=which):
                act(border_copy(s, which))

    tok_x[0].start()
    start(in_y)
    start(tok_x[1:])
    start(tok_local)
    start(small_local)
    start(in_local)
    start(in_sib[:2])

    start(out_x)
    start(out_y)
    start(out_local)

    def normalized(rows):
        values = rows.astype(jnp.float32)
        mean = jnp.mean(values * values, axis=-1, keepdims=True)
        return (values * lax.rsqrt(mean + norm_eps) * gain[...]).astype(jnp.bfloat16)

    def normalize(s, which):
        step_rows = 64

        def step(i, carry):
            at = pl.ds(pl.multiple_of(i * step_rows, step_rows), step_rows)
            rows_ref[s, which, at] = normalized(rows_ref[s, which, at])
            return carry

        lax.fori_loop(0, half // step_rows, step, 0)

    def project(values, kind, low=0, high=cols):
        return jnp.dot(
            values, w_in[kind, :, low:high], preferred_element_type=jnp.float32
        ).astype(jnp.bfloat16)

    def project_heads(s, which, kind, low, high):
        result = project(rows_ref[s, which], kind, low, high)
        at = span(z, x if which == 0 else other_x)
        for h in range(low // HEAD_DIM, high // HEAD_DIM):
            heads[kind, s, h, at] = result[:, h * HEAD_DIM - low : (h + 1) * HEAD_DIM - low]

    def span(owner_z, owner_x):
        return pl.ds(pl.multiple_of(owner_z * block + owner_x * half, half), half)

    for copy in tok_local + small_local:
        copy.wait()
    for s in range(seqs):
        normalize(s, 0)

    def weights_landed(k):
        in_y[k].wait_recv()
        if k < len(shared):
            in_z[k].start()
        in_corner[k].start()

    def weights_ready(k):
        in_local[k].wait()
        in_sib[k].wait_recv()
        if k < len(shared):
            in_z[k].wait_recv()
            in_corner_other[k].start()
            in_corner_other[k].wait_recv()
        in_corner[k].wait_recv()

    def z_copy(group, kinds, dest, which, which_seqs, first, last):
        at = span(z, x if which == 0 else other_x)
        view = heads.at[kinds, which_seqs, first:last, at]
        return pltpu.make_async_remote_copy(
            src_ref=view,
            dst_ref=view,
            send_sem=z_send.at[group, dest if last - first == 1 else z_count],
            recv_sem=z_recv.at[group, z if last - first == 1 else z_count],
            device_id={"sp": dest},
            device_id_type=MESH,
        )

    def queries_go(dest):
        return z >= z_count // 2

    everything = pl.ds(0, seqs)
    groups_z = []
    for kind in (KEY, VALUE):
        groups_z.append((pl.ds(kind, 1), 0, everything))
    for s in range(seqs):
        groups_z.append((pl.ds(QUERY, 1), 0, pl.ds(s, 1)))
    for s in range(seqs):
        groups_z.append((pl.ds(KEY, 2), 1, pl.ds(s, 1)))
        groups_z.append((pl.ds(QUERY, 1), 1, pl.ds(s, 1)))
    own_query = [2 + s for s in range(seqs)]
    other_pair = [2 + seqs + 2 * s for s in range(seqs)]
    other_query = [3 + seqs + 2 * s for s in range(seqs)]
    asks = [g in own_query or g in other_query for g in range(len(groups_z))]
    middle = z_count // 2

    def each_send(group, dests, act):
        kinds, which, which_seqs = groups_z[group]
        for dest in dests:
            going = z != dest
            if asks[group]:
                going = going & queries_go(dest)
            else:
                going = going & (z > 0)

            @pl.when(going)
            def to(dest=dest):
                act(z_copy(group, kinds, dest, which, which_seqs, dest, dest + 1))

        if not asks[group] and dests[0] >= middle:

            @pl.when(z == 0)
            def to_next():
                act(z_copy(group, kinds, 1, which, which_seqs, 0, z_count))

    def each_recv(group, sources):
        kinds, which, which_seqs = groups_z[group]
        for source in sources:
            if asks[group] and source < middle:
                continue
            coming = z != source
            if source == 0:
                coming = coming & (z >= middle)

            @pl.when(coming)
            def came(source=source):
                view = heads.at[kinds, which_seqs, 0:1, pl.ds(0, half)]
                pltpu.make_async_copy(view, view, z_recv.at[group, source]).wait()

    def pass_copy(group, dest):
        kinds, which, which_seqs = groups_z[group]
        at = span(0, x if which == 0 else other_x)
        view = heads.at[kinds, which_seqs, dest : dest + 1, at]
        return pltpu.make_async_remote_copy(
            src_ref=view,
            dst_ref=view,
            send_sem=pass_send.at[group, dest - middle],
            recv_sem=z_recv.at[group, 0],
            device_id={"sp": dest},
            device_id_type=MESH,
        )

    def pass_on(group):
        kinds, which, which_seqs = groups_z[group]

        @pl.when(z == 1)
        def from_first():
            view = heads.at[kinds, which_seqs, 0:z_count, pl.ds(0, half)]
            pltpu.make_async_copy(view, view, z_recv.at[group, z_count]).wait()
            for dest in right_dests:
                pass_copy(group, dest).start()

    left_dests = tuple(range(middle))
    right_dests = tuple(range(z_count - 1, middle - 1, -1))

    weights_landed(0)
    for number, (kind, low, high) in enumerate(pieces[:-1]):
        if number + 1 < len(shared):
            weights_landed(number + 1)
        if number + 2 < len(pieces):
            in_sib[number + 2].start()
        if number >= len(shared):
            weights_landed(number)
        weights_ready(number)

        def own_step(s, carry, kind=kind, low=low, high=high):
            project_heads(s, 0, kind, low, high)
            return carry

        lax.fori_loop(0, seqs, own_step, 0)
        group = own_query[0] if kind == QUERY else kind
        each_send(group, left_dests if low == 0 else right_dests, lambda copy: copy.start())
        if kind > KEY and low > 0:
            pass_on(kind - 1)

    def other_rows(s):
        tok_x[s].wait_recv()
        normalize(s, 1)
        each_border(s, lambda copy: copy.start())
        for group, kinds in ((other_pair[s], (KEY, VALUE)), (other_query[s], (QUERY,))):

            def other_step(kind, carry, s=s):
                project_heads(s, 1, kind, 0, cols)
                return carry

            lax.fori_loop(kinds[0], kinds[-1] + 1, other_step, 0)
            each_send(group, left_dests, lambda copy: copy.start())
            each_send(group, right_dests, lambda copy: copy.start())

    @pl.when(z == 0)
    def no_border():
        extended[:, 0:edge] = jnp.zeros((seqs, edge, cols), jnp.float32)

    def take_border(s):
        @pl.when(z > 0)
        def take():
            border_copy(s, 0).wait_recv()
            extended[s, 0:edge] = project(border[s], POOL).astype(jnp.float32)

    groups = cols // GROUP_WIDTH
    own_lanes = pl.ds(pl.multiple_of(x * cols, cols), cols)
    pool_copies = [
        remote(
            pool_tmp.at[s, pl.ds(pl.multiple_of(other_x * half, half), half)],
            pool_rows.at[s, :, own_lanes],
            {"tp": other_x},
        )
        for s in range(seqs)
    ]

    def pool_branch_rows(s):
        for which, owner in ((0, x), (1, other_x)):
            at = pl.multiple_of(edge + owner * half, edge)
            extended[s, pl.ds(at, half)] = project(rows_ref[s, which], POOL).astype(jnp.float32)
        seen = (
            z * block + lax.broadcasted_iota(jnp.int32, (block, GROUP_WIDTH), 0) + 1
        ).astype(jnp.float32)
        for g in range(groups):
            at = slice(g * GROUP_WIDTH, (g + 1) * GROUP_WIDTH)
            plain = extended[s, :, at]
            total = plain
            for doubling in range(g + 1):
                total = total + pltpu.roll(total, 2**doubling, 0)
            averaged = total[edge:] / jnp.minimum(seen, float(2 ** (g + 1)))
            departure = (averaged - plain[edge:]).astype(jnp.bfloat16)
            mixed = jnp.dot(departure, mix[x * groups + g], preferred_element_type=jnp.float32)
            pool_tmp[s, :, at] = (mixed * scale[x * groups + g]).astype(jnp.bfloat16)
        pool_rows[s, :, own_lanes] = pool_tmp[s, pl.ds(pl.multiple_of(x * half, half), half)]
        pool_copies[s].start()

    def head_lanes(owner_x, head):
        at = pl.multiple_of((owner_x * z_count + head) * HEAD_DIM, HEAD_DIM)
        return pl.ds(at, HEAD_DIM)

    def attn_slot(index, head):
        return head if index == 0 else z_count + head if index == 1 else 2 * z_count + index - 2

    def attn_copy(s, index, head, dest_x):
        first = index * block + dest_x * half
        return pltpu.make_async_remote_copy(
            src_ref=attn_own.at[s, head, first : first + half],
            dst_ref=attn_rows.at[s, :, head_lanes(x, head)],
            send_sem=attn_send.at[s, attn_slot(index, head), dest_x],
            recv_sem=attn_recv.at[s, x * z_count + head],
            device_id={"sp": index, "tp": dest_x},
            device_id_type=MESH,
        )

    def attention_block(s, index, head):
        low = index * block
        high = low + block
        query = heads[QUERY, s, head, low:high]
        gate = jnp.transpose(
            jnp.broadcast_to(gates[s, pl.ds(head, 1), low:high], (HEAD_DIM, block))
        )[:, :1]
        gate = gate * log2_e

        def scored(first, last):
            scores = lax.dot_general(
                query,
                heads[KEY, s, head, first:last],
                (((1,), (1,)), ((), ())),
                preferred_element_type=jnp.float32,
            )
            row = gates[s, pl.ds(head, 1), first:last] * log2_e
            return scores * (HEAD_DIM ** (-0.5) * log2_e) + (gate - row)

        def weighted(scores, top, first, last):
            lifted = jnp.exp2(scores - top)
            return jnp.sum(lifted, axis=1, keepdims=True), jnp.dot(
                lifted.astype(jnp.bfloat16),
                heads[VALUE, s, head, first:last],
                preferred_element_type=jnp.float32,
            )

        newest = scored(low, high)
        below = lax.broadcasted_iota(jnp.int32, newest.shape, 1) <= lax.broadcasted_iota(
            jnp.int32, newest.shape, 0
        )
        newest = jnp.where(below, newest, masked_score)
        top = jnp.max(newest, axis=1, keepdims=True)
        if low > 0:
            before = scored(0, low)
            top = jnp.maximum(top, jnp.max(before, axis=1, keepdims=True))
        denominator, total = weighted(newest, top, low, high)
        if low > 0:
            more_sum, more_total = weighted(before, top, 0, low)
            denominator = denominator + more_sum
            total = total + more_total
        attn_own[s, head, low:high] = (total / denominator).astype(jnp.bfloat16)

    def attention_rows(s, index, first_head, last_head, later=False):
        def head_step(head, carry):
            attention_block(s, index, head)
            for dest_x in range(2):
                here = (z == index) & (x == dest_x)

                going = z != index if later else jnp.logical_not(here)

                @pl.when(going)
                def send(dest_x=dest_x):
                    attn_copy(s, index, head, dest_x).start()

                @pl.when(here)
                def keep(dest_x=dest_x):
                    first = index * block + dest_x * half
                    attn_rows[s, :, head_lanes(x, head)] = attn_own[
                        s, head, first : first + half
                    ]

            return carry

        lax.fori_loop(first_head, last_head, head_step, 0)

    def heads_of(index):
        if index == 0:
            return 0, z_count
        if index == 1:
            return 0, z_count
        return z, z + 1

    def first_rows(s):
        later = 0 < s == seqs - 1
        for index in range(2):
            pl.when(z == index)(
                lambda index=index: attention_rows(s, index, *heads_of(index), later=later)
            )

    def first_rows_across(s):
        for index in range(2):
            for dest_x in range(2):

                @pl.when((z == index) & (x != dest_x))
                def across_x(index=index, dest_x=dest_x):
                    for head in range(z_count):
                        attn_copy(s, index, head, dest_x).start()

    def later_rows(s):
        arriving = ((KEY, VALUE) if s == 0 else ()) + (own_query[s], other_pair[s], other_query[s])
        for group in arriving:
            each_recv(group, range(middle))
        for index in range(middle, z_count):
            for group in arriving:
                each_recv(group, (index,))
            if s == 0 and index == middle:
                forward_half(1)
            attention_rows(s, index, *heads_of(index))

    def forward_half(kind):
        out_x[kind].wait_recv()
        out_xy[kind].start()
        out_xs[kind].start()

    for s in range(seqs):
        other_rows(s)
        if s + 1 < seqs:
            each_send(own_query[s + 1], left_dests, lambda copy: copy.start())
            each_send(own_query[s + 1], right_dests, lambda copy: copy.start())
        if s == 0:
            start(out_sib)
            weights_landed(len(pieces) - 1)
            weights_ready(len(pieces) - 1)
        take_border(s)
        pool_branch_rows(s)
        if s < seqs - 1:
            pass_on(other_pair[s])
    for s in range(seqs):
        if s == seqs - 1:
            forward_half(0)
            pass_on(other_pair[s])
        first_rows(s)

    for s in range(seqs):
        later_rows(s)
        if 0 < s == seqs - 1:
            first_rows_across(s)
        if s == 0:
            arrive(out_y)
            start(out_ys)

    out_xy[0].wait_recv()
    out_xys[0].start()
    for group in (tok_x, in_y, in_sib, in_corner, in_z, in_corner_other, out_x, out_y, out_sib):
        for copy in group:
            copy.wait_send()
    for s in range(seqs):
        each_border(s, lambda copy: copy.wait_send())

    for group in range(len(groups_z)):
        if not asks[group]:
            for dest in right_dests:
                pl.when(z == 1)(lambda group=group, dest=dest: pass_copy(group, dest).wait_send())
        each_send(group, left_dests, lambda copy: copy.wait_send())
        each_send(group, right_dests, lambda copy: copy.wait_send())
    for copy in out_local:
        copy.wait()

    arrive(out_xy[1:])
    start(out_xys[1:])
    arrive(out_xs)
    arrive(out_ys)
    arrive(out_sib)
    arrive(pool_copies)

    tiles = [f, sibling, across, f + 2 - 4 * (f // 2) + 1 - 2 * lax.rem(f, 2)]

    def tile_lanes(tile):
        return pl.ds(pl.multiple_of(tile * depth, depth), depth)

    def pool_part(s, tile):
        return jnp.dot(
            pool_rows[s], w_out[0, :, tile_lanes(tile)], preferred_element_type=jnp.float32
        )

    def attn_part(s, tile):
        return jnp.dot(
            attn_rows[s], w_out[1, :, tile_lanes(tile)], preferred_element_type=jnp.float32
        )

    def attn_side(s, tile, side):
        at = pl.ds(pl.multiple_of(side * cols, cols), cols)
        return jnp.dot(
            attn_rows[s, :, at],
            w_out[1, at, tile_lanes(tile)],
            preferred_element_type=jnp.float32,
        )

    def own_side_came(s):
        for head in range(z_count):

            @pl.when(jnp.logical_not((z < 2) | (z == head)))
            def came(head=head):
                view = attn_rows.at[s, :, 0:HEAD_DIM]
                pltpu.make_async_copy(view, view, attn_recv.at[s, x * z_count + head]).wait()

    def other_side_came(s):
        for head in range(z_count):
            view = attn_rows.at[s, :, 0:HEAD_DIM]
            pltpu.make_async_copy(view, view, attn_recv.at[s, other_x * z_count + head]).wait()

    def attention_came(s):
        own_side_came(s)
        other_side_came(s)

    for s in range(seqs):
        for number, tile in enumerate(tiles):
            if s == 0 and number == len(tiles) - 1:
                arrive(out_xys)
            pooled[s, :, tile_lanes(tile)] = pool_part(s, tile)
    last = seqs - 1
    for s in range(last):
        attention_came(s)
        for tile in tiles:
            result = pooled[s, :, tile_lanes(tile)] + attn_part(s, tile)
            out[s, :, tile_lanes(tile)] = result.astype(jnp.bfloat16)
    own_side_came(last)
    for tile in tiles:
        pooled[last, :, tile_lanes(tile)] += attn_side(last, tile, x)
    other_side_came(last)
    for tile in tiles:
        result = pooled[last, :, tile_lanes(tile)] + attn_side(last, tile, other_x)
        out[last, :, tile_lanes(tile)] = result.astype(jnp.bfloat16)

    for group in (
        out_xy, out_xs, out_ys, out_xys,
        pool_copies,
    ):
        for copy in group:
            copy.wait_send()

    def attention_sent(s, index):
        def head_step(head, carry):
            for dest_x in range(2):

                @pl.when(jnp.logical_not((z == index) & (x == dest_x)))
                def sent(dest_x=dest_x):
                    attn_copy(s, index, head, dest_x).wait_send()

            return carry

        lax.fori_loop(*heads_of(index), head_step, 0)

    for s in range(seqs):
        pl.when(z == 0)(lambda s=s: attention_sent(s, 0))
        pl.when(z == 1)(lambda s=s: attention_sent(s, 1))
        for index in range(2, z_count):
            attention_sent(s, index)


def fast_device(
    tokens,
    norm_gain,
    w_pool_in,
    pool_mix,
    pool_scale,
    w_query,
    w_key,
    w_value,
    gate_cache,
    w_out_pool,
    w_out_attn,
):
    seqs, half, width = tokens.shape
    block = 2 * half
    cols = w_key.shape[1]
    z_count = lax.axis_size("sp")
    length = block * z_count
    edge = 16
    bf16 = jnp.bfloat16
    anywhere = pl.BlockSpec(memory_space=pl.ANY)
    inside = pl.BlockSpec(memory_space=pltpu.VMEM)
    dma = pltpu.SemaphoreType.DMA
    return pl.pallas_call(
        layer_kernel,
        in_specs=[anywhere] * 11,
        out_specs=inside,
        out_shape=pltpu.VMEM(tokens.shape, bf16),
        scratch_shapes=[
            pltpu.VMEM((1, width), jnp.float32),
            pltpu.VMEM(pool_mix.shape, bf16),
            pltpu.VMEM((pool_mix.shape[0], 1, GROUP_WIDTH), jnp.float32),
            pltpu.VMEM(gate_cache.shape, jnp.float32),
            pltpu.VMEM((4, width, cols), bf16),
            pltpu.VMEM((2, 2 * cols, width), bf16),
            pltpu.VMEM((seqs, 2, half, width), bf16),
            pltpu.VMEM((3, seqs, z_count, length, HEAD_DIM), bf16),
            pltpu.VMEM((seqs, edge + block, cols), jnp.float32),
            pltpu.VMEM((seqs, edge, width), bf16),
            pltpu.VMEM((seqs, block, cols), bf16),
            pltpu.VMEM((seqs, half, 2 * cols), bf16),
            pltpu.VMEM((seqs, z_count, length, HEAD_DIM), bf16),
            pltpu.VMEM((seqs, half, 2 * cols), bf16),
            pltpu.VMEM((seqs, half, width), jnp.float32),
            dma((13 + seqs,)),
            dma((39 + 2 * seqs,)),
            dma((39 + 2 * seqs,)),
            dma((2 + 3 * seqs, z_count + 1)),
            dma((2 + 3 * seqs, z_count + 1)),
            dma((seqs, 2 * z_count + 2, 2)),
            dma((seqs, 2 * z_count)),
            dma((2, seqs)),
            dma((2 + 3 * seqs, z_count // 2)),
        ],
        compiler_params=pltpu.CompilerParams(
            collective_id=0,
            has_side_effects=True,
            vmem_limit_bytes=54 * 1024 * 1024,
        ),
    )(
        tokens,
        norm_gain.reshape(1, width),
        w_pool_in,
        pool_mix,
        pool_scale.reshape(-1, 1, GROUP_WIDTH),
        w_query,
        w_key,
        w_value,
        gate_cache,
        w_out_pool,
        w_out_attn,
    )


def on_device(*args):
    cols = args[5].shape[1]
    half = args[0].shape[1]
    sp_count = lax.axis_size("sp")
    suited = (
        lax.axis_size("tp") == 2
        and lax.axis_size("fs") == 4
        and cols == sp_count * HEAD_DIM
        and args[2].shape[1] == cols == 4 * GROUP_WIDTH
        and half % 128 == 0
        and args[0].shape[2] == 4 * cols
        and half * 2 * sp_count <= 2048
        and sp_count == 4
        and args[0].shape[0] <= 2
    )
    if suited:
        return fast_device(*args)
    return general_device(*args)


def solution(mesh):
    placed = (
        P("fs", ("sp", "tp"), None),
        P(),
        P("fs", "tp"),
        P(),
        P(),
        P("fs", "tp"),
        P("fs", "tp"),
        P("fs", "tp"),
        P("fs", "tp", None),
        P("tp", "fs"),
        P("tp", "fs"),
    )
    return jax.shard_map(
        on_device,
        mesh=mesh,
        in_specs=placed,
        out_specs=P("fs", ("sp", "tp"), None),
        check_vma=False,
    )
```

```python
import jax
import jax.numpy as jnp
from jax import lax
from jax.experimental import pallas as pl
from jax.experimental.pallas import tpu as pltpu
from jax.sharding import PartitionSpec as P

HEAD_DIM = 128
GROUP_WIDTH = 128


norm_eps = 1e-06
widest = 16
masked_score = -1e30


def shifted(x, axis, by):
    length = lax.axis_size(axis)
    pairs = [(i, i + by) for i in range(length) if 0 <= i + by < length]
    return lax.ppermute(x, axis, pairs)


def window_sums(extended):
    outcome = []
    current = extended
    offset = 1
    for doubling in range(4):
        padding = jnp.zeros((offset, extended.shape[1]), jnp.float32)
        current = current + jnp.concatenate([padding, current[:-offset]], axis=0)
        offset = offset * 2
        outcome.append(current[widest - 1 :])
    return outcome


def pool_branch(projected, border, first_group, first_position, mixing, scaling):
    row_count = projected.shape[0]
    channels = projected.shape[1]
    widened = projected.astype(jnp.float32)
    totals = window_sums(jnp.concatenate([border.astype(jnp.float32), widened], axis=0))
    token_positions = first_position + jnp.arange(row_count)
    window_index = (first_group + jnp.arange(channels) // GROUP_WIDTH) % 4
    averaged = jnp.zeros((row_count, channels), jnp.float32)
    for doubling in range(4):
        counted = jnp.minimum(token_positions + 1, 2 ** (doubling + 1)).astype(jnp.float32)
        picked = (window_index == doubling).astype(jnp.float32)
        averaged = averaged + picked[None, :] * totals[doubling] / counted[:, None]
    departure = (averaged - widened).astype(jnp.bfloat16)
    group_count = channels // GROUP_WIDTH
    mixed_rows = jnp.einsum(
        "tgc,gcd->tgd",
        departure.reshape(row_count, group_count, GROUP_WIDTH),
        mixing,
        preferred_element_type=jnp.float32,
    )
    return (mixed_rows.reshape(row_count, channels) * scaling[None, :]).astype(jnp.bfloat16)


def general_device(
    tokens,
    norm_gain,
    w_pool_in,
    pool_mix,
    pool_scale,
    w_query,
    w_key,
    w_value,
    gate_cache,
    w_out_pool,
    w_out_attn,
):
    tp_index = lax.axis_index("tp")
    tp_count = lax.axis_size("tp")
    seq_count = tokens.shape[0]
    own_count = tokens.shape[1]
    token_count = own_count * tp_count
    first_position = lax.axis_index("sp") * token_count
    own_rows = tokens.astype(jnp.float32)
    normed = (
        own_rows
        * lax.rsqrt(jnp.mean(own_rows * own_rows, axis=-1, keepdims=True) + norm_eps)
        * norm_gain[None, None, :]
    ).astype(jnp.bfloat16)
    pool_full, query_full, key_full, value_full, out_pool_full, out_attn_full = (
        lax.all_gather(w_pool_in, "fs", axis=0, tiled=True),
        lax.all_gather(w_query, "fs", axis=0, tiled=True),
        lax.all_gather(w_key, "fs", axis=0, tiled=True),
        lax.all_gather(w_value, "fs", axis=0, tiled=True),
        lax.all_gather(w_out_pool, "fs", axis=1, tiled=True),
        lax.all_gather(w_out_attn, "fs", axis=1, tiled=True),
    )
    pool_cols = w_pool_in.shape[1]
    attn_cols = w_query.shape[1]
    shard_rows = lax.all_gather(normed, "tp", axis=1, tiled=True)
    projected = jnp.concatenate(
        [
            jnp.dot(shard_rows, pool_full, preferred_element_type=jnp.float32).astype(jnp.bfloat16),
            jnp.dot(shard_rows, query_full, preferred_element_type=jnp.float32).astype(
                jnp.bfloat16
            ),
            jnp.dot(shard_rows, key_full, preferred_element_type=jnp.float32).astype(jnp.bfloat16),
            jnp.dot(shard_rows, value_full, preferred_element_type=jnp.float32).astype(
                jnp.bfloat16
            ),
        ],
        axis=2,
    )
    pool_in = projected[:, :, :pool_cols]
    query_proj = projected[:, :, pool_cols : pool_cols + attn_cols]
    key_proj = projected[:, :, pool_cols + attn_cols : pool_cols + 2 * attn_cols]
    value_proj = projected[:, :, pool_cols + 2 * attn_cols :]
    group_local = pool_cols // GROUP_WIDTH
    mixing = lax.dynamic_slice_in_dim(pool_mix, tp_index * group_local, group_local, 0)
    scaling = lax.dynamic_slice_in_dim(pool_scale, tp_index * pool_cols, pool_cols, 0)
    borders = shifted(pool_in[:, token_count - (widest - 1) :], "sp", 1)
    pool_out = jnp.stack(
        [
            pool_branch(
                pool_in[member],
                borders[member],
                tp_index * group_local,
                first_position,
                mixing,
                scaling,
            )
            for member in range(seq_count)
        ],
        axis=0,
    )
    head_count = attn_cols // HEAD_DIM
    query_heads = query_proj.reshape(seq_count, token_count, head_count, HEAD_DIM)
    query_gates = jnp.transpose(
        lax.dynamic_slice_in_dim(gate_cache, first_position, token_count, 2), (0, 2, 1)
    )
    query_positions = first_position + jnp.arange(token_count)
    last_position = first_position + token_count - 1
    score_scale = HEAD_DIM ** (-0.5)
    start_state = (
        jnp.full((seq_count, token_count, head_count), masked_score, jnp.float32),
        jnp.zeros((seq_count, token_count, head_count), jnp.float32),
        jnp.zeros((seq_count, token_count, head_count, HEAD_DIM), jnp.float32),
    )
    key_shard = lax.all_gather(key_proj, "sp", axis=1, tiled=True)
    value_shard = lax.all_gather(value_proj, "sp", axis=1, tiled=True)
    key_total = key_shard.shape[1]
    block_rows = 512

    def one_block(block_state, block_index):
        key_start = block_index * block_rows

        def compute(inner_state):
            running_top, running_sum, running_out = inner_state
            key_block = lax.dynamic_slice_in_dim(key_shard, block_index * block_rows, block_rows, 1)
            value_block = lax.dynamic_slice_in_dim(
                value_shard, block_index * block_rows, block_rows, 1
            )
            key_block = key_block.reshape(seq_count, block_rows, head_count, HEAD_DIM)
            value_block = value_block.reshape(seq_count, block_rows, head_count, HEAD_DIM)
            key_gates = lax.dynamic_slice_in_dim(gate_cache, key_start, block_rows, 2)
            scores = (
                jnp.einsum(
                    "sqhd,skhd->sqhk", query_heads, key_block, preferred_element_type=jnp.float32
                )
                * score_scale
            )
            scores = scores + query_gates[:, :, :, None] - key_gates[:, None, :, :]
            allowed = ((key_start + jnp.arange(block_rows))[None, :] <= query_positions[:, None])[
                None, :, None, :
            ]
            scores = jnp.where(allowed, scores, masked_score)
            new_top = jnp.maximum(running_top, jnp.max(scores, axis=3))
            weights = jnp.where(allowed, jnp.exp(scores - new_top[:, :, :, None]), 0.0)
            shrink = jnp.exp(running_top - new_top)
            running_sum = running_sum * shrink + jnp.sum(weights, axis=3)
            running_out = running_out * shrink[:, :, :, None] + jnp.einsum(
                "sqhk,skhd->sqhd",
                weights.astype(jnp.bfloat16),
                value_block,
                preferred_element_type=jnp.float32,
            )
            return (new_top, running_sum, running_out)

        def unchanged(inner_state):
            return inner_state

        return (lax.cond(key_start <= last_position, compute, unchanged, block_state), None)

    result, unused = lax.scan(one_block, start_state, jnp.arange(key_total // block_rows))
    final_top, final_sum, final_out = result
    attn_out = (
        (final_out / final_sum[:, :, :, None])
        .astype(jnp.bfloat16)
        .reshape(seq_count, token_count, attn_cols)
    )
    pool_flat = jnp.transpose(
        pool_out.reshape(seq_count, tp_count, own_count, pool_cols), (1, 0, 2, 3)
    ).reshape(tp_count * seq_count * own_count, pool_cols)
    attn_flat = jnp.transpose(
        attn_out.reshape(seq_count, tp_count, own_count, attn_cols), (1, 0, 2, 3)
    ).reshape(tp_count * seq_count * own_count, attn_cols)
    summed = lax.psum_scatter(
        (
            jnp.dot(pool_flat, out_pool_full, preferred_element_type=jnp.float32)
            + jnp.dot(attn_flat, out_attn_full, preferred_element_type=jnp.float32)
        ).astype(jnp.bfloat16),
        "tp",
        scatter_dimension=0,
        tiled=True,
    ).astype(jnp.float32)
    return summed.astype(jnp.bfloat16).reshape(seq_count, own_count, summed.shape[1])


log2_e = 1.4426950408889634
MESH = pl.DeviceIdType.MESH
KEY, VALUE, QUERY, POOL = 0, 1, 2, 3


def layer_kernel(
    tokens,
    gain_in,
    w_pool,
    mix_in,
    scale_in,
    w_query,
    w_key,
    w_value,
    gates_in,
    w_out_pool,
    w_out_attn,
    out,
    gain,
    mix,
    scale,
    gates,
    w_in,
    w_out,
    rows_ref,
    heads,
    extended,
    border,
    pool_tmp,
    pool_rows,
    attn_own,
    attn_rows,
    pooled,
    local_sem,
    send_sem,
    recv_sem,
    z_send,
    z_recv,
    attn_send,
    attn_recv,
    border_sem,
    pass_send,
):
    z = lax.axis_index("sp")
    f = lax.axis_index("fs")
    x = lax.axis_index("tp")
    seqs, half, width = tokens.shape
    block = 2 * half
    depth, cols = w_key.shape
    other_x = 1 - x
    sibling = f + 1 - 2 * lax.rem(f, 2)
    across = lax.rem(f + 2, 4)
    z_count = heads.shape[2]
    edge = border.shape[1]

    def z_at(by):
        return lax.rem(z + by, z_count)

    barrier = pltpu.get_barrier_semaphore()
    peers = [{"tp": other_x}, {"fs": sibling}, {"fs": across}]
    for by in range(1, z_count):
        peers.append({"sp": z_at(by)})
        peers.append({"sp": z_at(by), "tp": other_x})
    for peer in peers:
        pl.semaphore_signal(barrier, inc=1, device_id=peer, device_id_type=MESH)
    pl.semaphore_wait(barrier, len(peers))

    numbers = iter(range(send_sem.shape[0]))

    def remote(source, target, peer):
        number = next(numbers)
        return pltpu.make_async_remote_copy(
            src_ref=source,
            dst_ref=target,
            send_sem=send_sem.at[number],
            recv_sem=recv_sem.at[number],
            device_id=peer,
            device_id_type=MESH,
        )

    local_numbers = iter(range(local_sem.shape[0]))

    def local(source, target):
        return pltpu.make_async_copy(source, target, local_sem.at[next(local_numbers)])

    def in_slot(piece, owner):
        kind, low, high = piece
        at = pl.multiple_of(owner * depth, depth)
        return w_in.at[kind, pl.ds(at, depth), low:high]

    def in_part(piece, owner, part):
        kind, low, high = piece
        at = pl.multiple_of(owner * depth + part * (depth // 2), depth // 2)
        return w_in.at[kind, pl.ds(at, depth // 2), low:high]

    def out_slot(kind, owner_x, owner_f):
        return w_out.at[
            kind,
            pl.ds(pl.multiple_of(owner_x * cols, cols), cols),
            pl.ds(pl.multiple_of(owner_f * depth, depth), depth),
        ]

    w_own = (w_key, w_value, w_query, w_pool)
    out_own = (w_out_pool, w_out_attn)
    pair = 2 * HEAD_DIM
    pieces = [
        (kind, low, low + pair) for kind in (KEY, VALUE, QUERY) for low in range(0, cols, pair)
    ]
    pieces.append((POOL, 0, cols))

    def own_piece(piece):
        kind, low, high = piece
        return w_own[kind].at[:, low:high]

    tok_x = [remote(tokens.at[s], rows_ref.at[s, 1], {"tp": other_x}) for s in range(seqs)]
    parity = lax.rem(z, 2)
    partner = z + 1 - 2 * parity
    shared = [p for p in pieces if p[0] == KEY]
    in_y = []
    in_z = []
    in_corner_other = []
    for p in pieces:
        if p in shared:
            kind, low, high = p
            at = pl.multiple_of(parity * (depth // 2), depth // 2)
            source = w_own[kind].at[pl.ds(at, depth // 2), low:high]
            in_y.append(remote(source, in_part(p, f, parity), {"fs": across}))
            view = in_part(p, across, parity)
            in_z.append(remote(view, view, {"sp": partner}))
            view = in_part(p, across, 1 - parity)
            in_corner_other.append(remote(view, view, {"fs": sibling}))
        else:
            in_y.append(remote(own_piece(p), in_slot(p, f), {"fs": across}))
    in_sib = [remote(own_piece(p), in_slot(p, f), {"fs": sibling}) for p in pieces]
    in_corner = []
    for p in pieces:
        view = in_part(p, across, parity) if p in shared else in_slot(p, across)
        in_corner.append(remote(view, view, {"fs": sibling}))
    out_x = [remote(out_own[k], out_slot(k, x, f), {"tp": other_x}) for k in range(2)]
    out_y = [remote(out_own[k], out_slot(k, x, f), {"fs": across}) for k in range(2)]
    out_sib = [remote(out_own[k], out_slot(k, x, f), {"fs": sibling}) for k in range(2)]

    def forwarded(owner_x, owner_f, peer):
        return [
            remote(out_slot(k, owner_x, owner_f), out_slot(k, owner_x, owner_f), peer)
            for k in range(2)
        ]

    out_xy = forwarded(other_x, f, {"fs": across})
    out_xs = forwarded(other_x, f, {"fs": sibling})
    out_ys = forwarded(x, across, {"fs": sibling})
    out_xys = forwarded(other_x, across, {"fs": sibling})
    small_local = [
        local(gain_in, gain),
        local(mix_in, mix),
        local(scale_in, scale),
        local(gates_in, gates),
    ]
    tok_local = [local(tokens.at[s], rows_ref.at[s, 0]) for s in range(seqs)]
    in_local = [local(own_piece(p), in_slot(p, f)) for p in pieces]
    out_local = [local(out_own[k], out_slot(k, x, f)) for k in range(2)]

    def start(copies):
        for copy in copies:
            copy.start()

    def arrive(copies):
        for copy in copies:
            copy.wait_recv()

    def border_copy(s, which):
        return pltpu.make_async_remote_copy(
            src_ref=rows_ref.at[s, which, half - edge :],
            dst_ref=border.at[s],
            send_sem=border_sem.at[0, s],
            recv_sem=border_sem.at[1, s],
            device_id={"sp": z_at(1)},
            device_id_type=MESH,
        )

    def each_border(s, act):
        for which, owner in ((0, 1), (1, 0)):

            @pl.when((z < z_count - 1) & (x == owner))
            def to_next(which=which):
                act(border_copy(s, which))

    tok_x[0].start()
    start(in_y)
    start(tok_x[1:])
    start(tok_local)
    start(small_local)
    start(in_local)
    start(in_sib[:2])

    start(out_x)
    start(out_y)
    start(out_local)

    def normalized(rows):
        values = rows.astype(jnp.float32)
        mean = jnp.mean(values * values, axis=-1, keepdims=True)
        return (values * lax.rsqrt(mean + norm_eps) * gain[...]).astype(jnp.bfloat16)

    def normalize(s, which):
        step_rows = 64

        def step(i, carry):
            at = pl.ds(pl.multiple_of(i * step_rows, step_rows), step_rows)
            rows_ref[s, which, at] = normalized(rows_ref[s, which, at])
            return carry

        lax.fori_loop(0, half // step_rows, step, 0)

    def project(values, kind, low=0, high=cols):
        return jnp.dot(
            values, w_in[kind, :, low:high], preferred_element_type=jnp.float32
        ).astype(jnp.bfloat16)

    def project_heads(s, which, kind, low, high):
        result = project(rows_ref[s, which], kind, low, high)
        at = span(z, x if which == 0 else other_x)
        for h in range(low // HEAD_DIM, high // HEAD_DIM):
            heads[kind, s, h, at] = result[:, h * HEAD_DIM - low : (h + 1) * HEAD_DIM - low]

    def span(owner_z, owner_x):
        return pl.ds(pl.multiple_of(owner_z * block + owner_x * half, half), half)

    for copy in tok_local + small_local:
        copy.wait()
    for s in range(seqs):
        normalize(s, 0)

    def weights_landed(k):
        in_y[k].wait_recv()
        if k < len(shared):
            in_z[k].start()
        in_corner[k].start()

    def weights_ready(k):
        in_local[k].wait()
        in_sib[k].wait_recv()
        if k < len(shared):
            in_z[k].wait_recv()
            in_corner_other[k].start()
            in_corner_other[k].wait_recv()
        in_corner[k].wait_recv()

    def z_copy(group, kinds, dest, which, which_seqs, first, last):
        at = span(z, x if which == 0 else other_x)
        view = heads.at[kinds, which_seqs, first:last, at]
        return pltpu.make_async_remote_copy(
            src_ref=view,
            dst_ref=view,
            send_sem=z_send.at[group, dest if last - first == 1 else z_count],
            recv_sem=z_recv.at[group, z if last - first == 1 else z_count],
            device_id={"sp": dest},
            device_id_type=MESH,
        )

    def queries_go(dest):
        return z >= z_count // 2

    everything = pl.ds(0, seqs)
    groups_z = []
    for kind in (KEY, VALUE):
        groups_z.append((pl.ds(kind, 1), 0, everything))
    for s in range(seqs):
        groups_z.append((pl.ds(QUERY, 1), 0, pl.ds(s, 1)))
    for s in range(seqs):
        groups_z.append((pl.ds(KEY, 2), 1, pl.ds(s, 1)))
        groups_z.append((pl.ds(QUERY, 1), 1, pl.ds(s, 1)))
    own_query = [2 + s for s in range(seqs)]
    other_pair = [2 + seqs + 2 * s for s in range(seqs)]
    other_query = [3 + seqs + 2 * s for s in range(seqs)]
    asks = [g in own_query or g in other_query for g in range(len(groups_z))]
    middle = z_count // 2

    def each_send(group, dests, act):
        kinds, which, which_seqs = groups_z[group]
        for dest in dests:
            going = z != dest
            if asks[group]:
                going = going & queries_go(dest)
            else:
                going = going & (z > 0)

            @pl.when(going)
            def to(dest=dest):
                act(z_copy(group, kinds, dest, which, which_seqs, dest, dest + 1))

        if not asks[group] and dests[0] >= middle:

            @pl.when(z == 0)
            def to_next():
                act(z_copy(group, kinds, 1, which, which_seqs, 0, z_count))

    def each_recv(group, sources):
        kinds, which, which_seqs = groups_z[group]
        for source in sources:
            if asks[group] and source < middle:
                continue
            coming = z != source
            if source == 0:
                coming = coming & (z >= middle)

            @pl.when(coming)
            def came(source=source):
                view = heads.at[kinds, which_seqs, 0:1, pl.ds(0, half)]
                pltpu.make_async_copy(view, view, z_recv.at[group, source]).wait()

    def pass_copy(group, dest):
        kinds, which, which_seqs = groups_z[group]
        at = span(0, x if which == 0 else other_x)
        view = heads.at[kinds, which_seqs, dest : dest + 1, at]
        return pltpu.make_async_remote_copy(
            src_ref=view,
            dst_ref=view,
            send_sem=pass_send.at[group, dest - middle],
            recv_sem=z_recv.at[group, 0],
            device_id={"sp": dest},
            device_id_type=MESH,
        )

    def pass_on(group):
        kinds, which, which_seqs = groups_z[group]

        @pl.when(z == 1)
        def from_first():
            view = heads.at[kinds, which_seqs, 0:z_count, pl.ds(0, half)]
            pltpu.make_async_copy(view, view, z_recv.at[group, z_count]).wait()
            for dest in right_dests:
                pass_copy(group, dest).start()

    left_dests = tuple(range(middle))
    right_dests = tuple(range(z_count - 1, middle - 1, -1))

    weights_landed(0)
    for number, (kind, low, high) in enumerate(pieces[:-1]):
        if number + 1 < len(shared):
            weights_landed(number + 1)
        if number + 2 < len(pieces):
            in_sib[number + 2].start()
        if number >= len(shared):
            weights_landed(number)
        weights_ready(number)

        def own_step(s, carry, kind=kind, low=low, high=high):
            project_heads(s, 0, kind, low, high)
            return carry

        lax.fori_loop(0, seqs, own_step, 0)
        group = own_query[0] if kind == QUERY else kind
        each_send(group, left_dests if low == 0 else right_dests, lambda copy: copy.start())
        if kind > KEY and low > 0:
            pass_on(kind - 1)

    def other_rows(s):
        tok_x[s].wait_recv()
        normalize(s, 1)
        each_border(s, lambda copy: copy.start())
        for group, kinds in ((other_pair[s], (KEY, VALUE)), (other_query[s], (QUERY,))):

            def other_step(kind, carry, s=s):
                project_heads(s, 1, kind, 0, cols)
                return carry

            lax.fori_loop(kinds[0], kinds[-1] + 1, other_step, 0)
            each_send(group, left_dests, lambda copy: copy.start())
            each_send(group, right_dests, lambda copy: copy.start())

    @pl.when(z == 0)
    def no_border():
        extended[:, 0:edge] = jnp.zeros((seqs, edge, cols), jnp.float32)

    def take_border(s):
        @pl.when(z > 0)
        def take():
            border_copy(s, 0).wait_recv()
            extended[s, 0:edge] = project(border[s], POOL).astype(jnp.float32)

    groups = cols // GROUP_WIDTH
    own_lanes = pl.ds(pl.multiple_of(x * cols, cols), cols)
    pool_copies = [
        remote(
            pool_tmp.at[s, pl.ds(pl.multiple_of(other_x * half, half), half)],
            pool_rows.at[s, :, own_lanes],
            {"tp": other_x},
        )
        for s in range(seqs)
    ]

    def pool_branch_rows(s):
        for which, owner in ((0, x), (1, other_x)):
            at = pl.multiple_of(edge + owner * half, edge)
            extended[s, pl.ds(at, half)] = project(rows_ref[s, which], POOL).astype(jnp.float32)
        seen = (
            z * block + lax.broadcasted_iota(jnp.int32, (block, GROUP_WIDTH), 0) + 1
        ).astype(jnp.float32)
        for g in range(groups):
            at = slice(g * GROUP_WIDTH, (g + 1) * GROUP_WIDTH)
            plain = extended[s, :, at]
            total = plain
            for doubling in range(g + 1):
                total = total + pltpu.roll(total, 2**doubling, 0)
            averaged = total[edge:] / jnp.minimum(seen, float(2 ** (g + 1)))
            departure = (averaged - plain[edge:]).astype(jnp.bfloat16)
            mixed = jnp.dot(departure, mix[x * groups + g], preferred_element_type=jnp.float32)
            pool_tmp[s, :, at] = (mixed * scale[x * groups + g]).astype(jnp.bfloat16)
        pool_rows[s, :, own_lanes] = pool_tmp[s, pl.ds(pl.multiple_of(x * half, half), half)]
        pool_copies[s].start()

    def head_lanes(owner_x, head):
        at = pl.multiple_of((owner_x * z_count + head) * HEAD_DIM, HEAD_DIM)
        return pl.ds(at, HEAD_DIM)

    def attn_slot(index, head):
        return head if index == 0 else z_count + head if index == 1 else 2 * z_count + index - 2

    def attn_copy(s, index, head, dest_x):
        first = index * block + dest_x * half
        return pltpu.make_async_remote_copy(
            src_ref=attn_own.at[s, head, first : first + half],
            dst_ref=attn_rows.at[s, :, head_lanes(x, head)],
            send_sem=attn_send.at[s, attn_slot(index, head), dest_x],
            recv_sem=attn_recv.at[s, x * z_count + head],
            device_id={"sp": index, "tp": dest_x},
            device_id_type=MESH,
        )

    def attention_block(s, index, head):
        low = index * block
        high = low + block
        query = heads[QUERY, s, head, low:high]
        gate = jnp.transpose(
            jnp.broadcast_to(gates[s, pl.ds(head, 1), low:high], (HEAD_DIM, block))
        )[:, :1]
        gate = gate * log2_e

        def scored(first, last):
            scores = lax.dot_general(
                query,
                heads[KEY, s, head, first:last],
                (((1,), (1,)), ((), ())),
                preferred_element_type=jnp.float32,
            )
            row = gates[s, pl.ds(head, 1), first:last] * log2_e
            return scores * (HEAD_DIM ** (-0.5) * log2_e) + (gate - row)

        def weighted(scores, top, first, last):
            lifted = jnp.exp2(scores - top)
            return jnp.sum(lifted, axis=1, keepdims=True), jnp.dot(
                lifted.astype(jnp.bfloat16),
                heads[VALUE, s, head, first:last],
                preferred_element_type=jnp.float32,
            )

        newest = scored(low, high)
        below = lax.broadcasted_iota(jnp.int32, newest.shape, 1) <= lax.broadcasted_iota(
            jnp.int32, newest.shape, 0
        )
        newest = jnp.where(below, newest, masked_score)
        top = jnp.max(newest, axis=1, keepdims=True)
        if low > 0:
            before = scored(0, low)
            top = jnp.maximum(top, jnp.max(before, axis=1, keepdims=True))
        denominator, total = weighted(newest, top, low, high)
        if low > 0:
            more_sum, more_total = weighted(before, top, 0, low)
            denominator = denominator + more_sum
            total = total + more_total
        attn_own[s, head, low:high] = (total / denominator).astype(jnp.bfloat16)

    def attention_rows(s, index, first_head, last_head, later=False):
        def head_step(head, carry):
            attention_block(s, index, head)
            for dest_x in range(2):
                here = (z == index) & (x == dest_x)

                going = z != index if later else jnp.logical_not(here)

                @pl.when(going)
                def send(dest_x=dest_x):
                    attn_copy(s, index, head, dest_x).start()

                @pl.when(here)
                def keep(dest_x=dest_x):
                    first = index * block + dest_x * half
                    attn_rows[s, :, head_lanes(x, head)] = attn_own[
                        s, head, first : first + half
                    ]

            return carry

        lax.fori_loop(first_head, last_head, head_step, 0)

    def heads_of(index):
        if index == 0:
            return 0, z_count
        if index == 1:
            return 0, z_count
        return z, z + 1

    def first_rows(s):
        later = 0 < s == seqs - 1
        for index in range(2):
            pl.when(z == index)(
                lambda index=index: attention_rows(s, index, *heads_of(index), later=later)
            )

    def first_rows_across(s):
        for index in range(2):
            for dest_x in range(2):

                @pl.when((z == index) & (x != dest_x))
                def across_x(index=index, dest_x=dest_x):
                    for head in range(z_count):
                        attn_copy(s, index, head, dest_x).start()

    def later_rows(s):
        arriving = ((KEY, VALUE) if s == 0 else ()) + (own_query[s], other_pair[s], other_query[s])
        for group in arriving:
            each_recv(group, range(middle))
        if 0 < s == seqs - 1:
            for group in arriving:
                each_recv(group, range(middle, z_count))
            for index in range(z_count - 1, middle - 1, -1):
                attention_rows(s, index, *heads_of(index))
            return
        for index in range(middle, z_count):
            for group in arriving:
                each_recv(group, (index,))
            if s == 0 and index == middle:
                forward_half(1)
            attention_rows(s, index, *heads_of(index))

    def forward_half(kind):
        out_x[kind].wait_recv()
        out_xy[kind].start()
        out_xs[kind].start()

    for s in range(seqs):
        other_rows(s)
        if s + 1 < seqs:
            each_send(own_query[s + 1], left_dests, lambda copy: copy.start())
            each_send(own_query[s + 1], right_dests, lambda copy: copy.start())
        if s == 0:
            start(out_sib)
            weights_landed(len(pieces) - 1)
            weights_ready(len(pieces) - 1)
        take_border(s)
        pool_branch_rows(s)
        if s < seqs - 1:
            pass_on(other_pair[s])
    for s in range(seqs):
        if s == seqs - 1:
            forward_half(0)
            pass_on(other_pair[s])
        first_rows(s)

    for s in range(seqs):
        later_rows(s)
        if 0 < s == seqs - 1:
            first_rows_across(s)
        if s == 0:
            arrive(out_y)
            start(out_ys)

    out_xy[0].wait_recv()
    out_xys[0].start()
    for group in (tok_x, in_y, in_sib, in_corner, in_z, in_corner_other, out_x, out_y, out_sib):
        for copy in group:
            copy.wait_send()
    for s in range(seqs):
        each_border(s, lambda copy: copy.wait_send())

    for group in range(len(groups_z)):
        if not asks[group]:
            for dest in right_dests:
                pl.when(z == 1)(lambda group=group, dest=dest: pass_copy(group, dest).wait_send())
        each_send(group, left_dests, lambda copy: copy.wait_send())
        each_send(group, right_dests, lambda copy: copy.wait_send())
    for copy in out_local:
        copy.wait()

    arrive(out_xy[1:])
    start(out_xys[1:])
    arrive(out_xs)
    arrive(out_ys)
    arrive(out_sib)
    arrive(pool_copies)

    tiles = [f, sibling, across, f + 2 - 4 * (f // 2) + 1 - 2 * lax.rem(f, 2)]

    def tile_lanes(tile):
        return pl.ds(pl.multiple_of(tile * depth, depth), depth)

    def pool_part(s, tile):
        return jnp.dot(
            pool_rows[s], w_out[0, :, tile_lanes(tile)], preferred_element_type=jnp.float32
        )

    def attn_part(s, tile):
        return jnp.dot(
            attn_rows[s], w_out[1, :, tile_lanes(tile)], preferred_element_type=jnp.float32
        )

    def attn_side(s, tile, side):
        at = pl.ds(pl.multiple_of(side * cols, cols), cols)
        return jnp.dot(
            attn_rows[s, :, at],
            w_out[1, at, tile_lanes(tile)],
            preferred_element_type=jnp.float32,
        )

    def own_side_came(s):
        for head in range(z_count):

            @pl.when(jnp.logical_not((z < 2) | (z == head)))
            def came(head=head):
                view = attn_rows.at[s, :, 0:HEAD_DIM]
                pltpu.make_async_copy(view, view, attn_recv.at[s, x * z_count + head]).wait()

    def other_side_came(s):
        for head in range(z_count):
            view = attn_rows.at[s, :, 0:HEAD_DIM]
            pltpu.make_async_copy(view, view, attn_recv.at[s, other_x * z_count + head]).wait()

    def attention_came(s):
        own_side_came(s)
        other_side_came(s)

    for s in range(seqs):
        for number, tile in enumerate(tiles):
            if s == 0 and number == len(tiles) - 1:
                arrive(out_xys)
            pooled[s, :, tile_lanes(tile)] = pool_part(s, tile)
    last = seqs - 1
    for s in range(last):
        attention_came(s)
        for tile in tiles:
            result = pooled[s, :, tile_lanes(tile)] + attn_part(s, tile)
            out[s, :, tile_lanes(tile)] = result.astype(jnp.bfloat16)
    own_side_came(last)
    for tile in tiles:
        pooled[last, :, tile_lanes(tile)] += attn_side(last, tile, x)
    other_side_came(last)
    for tile in tiles:
        result = pooled[last, :, tile_lanes(tile)] + attn_side(last, tile, other_x)
        out[last, :, tile_lanes(tile)] = result.astype(jnp.bfloat16)

    for group in (
        out_xy, out_xs, out_ys, out_xys,
        pool_copies,
    ):
        for copy in group:
            copy.wait_send()

    def attention_sent(s, index):
        def head_step(head, carry):
            for dest_x in range(2):

                @pl.when(jnp.logical_not((z == index) & (x == dest_x)))
                def sent(dest_x=dest_x):
                    attn_copy(s, index, head, dest_x).wait_send()

            return carry

        lax.fori_loop(*heads_of(index), head_step, 0)

    for s in range(seqs):
        pl.when(z == 0)(lambda s=s: attention_sent(s, 0))
        pl.when(z == 1)(lambda s=s: attention_sent(s, 1))
        for index in range(2, z_count):
            attention_sent(s, index)


def fast_device(
    tokens,
    norm_gain,
    w_pool_in,
    pool_mix,
    pool_scale,
    w_query,
    w_key,
    w_value,
    gate_cache,
    w_out_pool,
    w_out_attn,
):
    seqs, half, width = tokens.shape
    block = 2 * half
    cols = w_key.shape[1]
    z_count = lax.axis_size("sp")
    length = block * z_count
    edge = 16
    bf16 = jnp.bfloat16
    anywhere = pl.BlockSpec(memory_space=pl.ANY)
    inside = pl.BlockSpec(memory_space=pltpu.VMEM)
    dma = pltpu.SemaphoreType.DMA
    return pl.pallas_call(
        layer_kernel,
        in_specs=[anywhere] * 11,
        out_specs=inside,
        out_shape=pltpu.VMEM(tokens.shape, bf16),
        scratch_shapes=[
            pltpu.VMEM((1, width), jnp.float32),
            pltpu.VMEM(pool_mix.shape, bf16),
            pltpu.VMEM((pool_mix.shape[0], 1, GROUP_WIDTH), jnp.float32),
            pltpu.VMEM(gate_cache.shape, jnp.float32),
            pltpu.VMEM((4, width, cols), bf16),
            pltpu.VMEM((2, 2 * cols, width), bf16),
            pltpu.VMEM((seqs, 2, half, width), bf16),
            pltpu.VMEM((3, seqs, z_count, length, HEAD_DIM), bf16),
            pltpu.VMEM((seqs, edge + block, cols), jnp.float32),
            pltpu.VMEM((seqs, edge, width), bf16),
            pltpu.VMEM((seqs, block, cols), bf16),
            pltpu.VMEM((seqs, half, 2 * cols), bf16),
            pltpu.VMEM((seqs, z_count, length, HEAD_DIM), bf16),
            pltpu.VMEM((seqs, half, 2 * cols), bf16),
            pltpu.VMEM((seqs, half, width), jnp.float32),
            dma((13 + seqs,)),
            dma((39 + 2 * seqs,)),
            dma((39 + 2 * seqs,)),
            dma((2 + 3 * seqs, z_count + 1)),
            dma((2 + 3 * seqs, z_count + 1)),
            dma((seqs, 2 * z_count + 2, 2)),
            dma((seqs, 2 * z_count)),
            dma((2, seqs)),
            dma((2 + 3 * seqs, z_count // 2)),
        ],
        compiler_params=pltpu.CompilerParams(
            collective_id=0,
            has_side_effects=True,
            vmem_limit_bytes=54 * 1024 * 1024,
        ),
    )(
        tokens,
        norm_gain.reshape(1, width),
        w_pool_in,
        pool_mix,
        pool_scale.reshape(-1, 1, GROUP_WIDTH),
        w_query,
        w_key,
        w_value,
        gate_cache,
        w_out_pool,
        w_out_attn,
    )


def on_device(*args):
    cols = args[5].shape[1]
    half = args[0].shape[1]
    sp_count = lax.axis_size("sp")
    suited = (
        lax.axis_size("tp") == 2
        and lax.axis_size("fs") == 4
        and cols == sp_count * HEAD_DIM
        and args[2].shape[1] == cols == 4 * GROUP_WIDTH
        and half % 128 == 0
        and args[0].shape[2] == 4 * cols
        and half * 2 * sp_count <= 2048
        and sp_count == 4
        and args[0].shape[0] <= 2
    )
    if suited:
        return fast_device(*args)
    return general_device(*args)


def solution(mesh):
    placed = (
        P("fs", ("sp", "tp"), None),
        P(),
        P("fs", "tp"),
        P(),
        P(),
        P("fs", "tp"),
        P("fs", "tp"),
        P("fs", "tp"),
        P("fs", "tp", None),
        P("tp", "fs"),
        P("tp", "fs"),
    )
    return jax.shard_map(
        on_device,
        mesh=mesh,
        in_specs=placed,
        out_specs=P("fs", ("sp", "tp"), None),
        check_vma=False,
    )
```
